128 devices in a mesh: sp: 64 (over z, y, x), tp: 2 (over core).
Axes of the slice: x: 4, y: 4, z: 4, core: 2. Of those that a mesh axis runs over, the one named last changes fastest.
Arguments:
- projected_queries: bfloat16 [32768, 1024], P('sp', 'tp'), may hold values from -6 to 6
- projected_keys: bfloat16 [32768, 1024], P('sp', 'tp'), may hold values from -6 to 6
- projected_values: bfloat16 [32768, 1024], P('sp', 'tp'), may hold values from -6 to 6
- output_gate_values: bfloat16 [32768, 1024], P('sp', 'tp'), may hold values from -6 to 6
- write_strength_logits: bfloat16 [32768, 8], P('sp', 'tp'), may hold values from -6.5 to 3
- decay_input_logits: bfloat16 [32768, 8], P('sp', 'tp'), may hold values from -5 to 5
- head_rate_logarithm: float32 [8], P('tp'), may hold values from -8 to 2.3
- extra_log_decay: float32 [32768, 8], P('sp', 'tp'), may hold values from -0.7 to 0
- per_head_norm_gain: float32 [128], replicated, may hold values from 0.1 to 1.9
- output_matrix: bfloat16 [1024, 2048], replicated, may hold values from -0.1875 to 0.1875
- residual: bfloat16 [32768, 2048], P(('sp', 'tp')), may hold values from -6 to 6
- mixture_norm_gain: float32 [2048], replicated, may hold values from 0.1 to 1.9
- selected_expert_index: int32 [32768, 4], P(('sp', 'tp')), may hold values from 0 to 127, all different within a row; in each aligned block of 256 rows (0 to 255, 256 to 511, ...) at most 12 rows name the same one
- routing_weight: float32 [32768, 4], P(('sp', 'tp')), may hold values from 0.1 to 0.9
- routed_gate_weight: bfloat16 [128, 2048, 512], P(('sp', 'tp')), may hold values from -0.125 to 0.125
- routed_up_weight: bfloat16 [128, 2048, 512], P(('sp', 'tp')), may hold values from -0.125 to 0.125
- routed_down_weight: bfloat16 [128, 512, 2048], P(('sp', 'tp')), may hold values from -0.25 to 0.25
- common_gate_weight: bfloat16 [2048, 512], replicated, may hold values from -0.125 to 0.125
- common_up_weight: bfloat16 [2048, 512], replicated, may hold values from -0.125 to 0.125
- common_down_weight: bfloat16 [512, 2048], replicated, may hold values from -0.25 to 0.25
Outputs:
- block_out: bfloat16 [32768, 2048], P(('sp', 'tp'))
The draws below stay inside these ranges and needn't reach their ends.
Inputs may be any that keep to these rules, and one draw needn't show every extreme that they name: `selected_expert_index`: each row names 4 different experts. Among the rows that one device holds, no expert is named more than 12 times.
All inputs are finite; a program needn't handle non-finite values.
Results may differ from the reference program's by a relative error of at most 0.008.
Values may be sent and summed in bfloat16 or wider, within the bound.
No kernel may reach another device: no remote copies, remote signals or barrier semaphores. Data moves between devices by JAX's collectives and lax.ppermute only.
A program may use at most 192 MiB of HBM per device.

```python
import math
import jax
import jax.numpy as jnp
import numpy as np
from jax import lax

D = 2048
HEADS = 8
HD = 128
EFF = 512
SFF = 512
TOP_K = 4
SPAN = 64
TOK_DEV = 512
TOKENS = 32768
EXPERTS = 128
CAP = 12
N_SP = 64
N_TP = 2


def head_order(key):
    return jax.random.permutation(jax.random.fold_in(key, 11), HEADS)


def draw_head_rate_logarithm(key, part):
    order = head_order(key)
    jitter = jax.random.uniform(jax.random.fold_in(key, 12), (HEADS,), jnp.float32, -0.4, 0.4)
    fast = order < HEADS // 2
    slow_level = math.log(244.0 / TOKENS)
    return jnp.where(fast, 1.8, slow_level).astype(jnp.float32) + jitter


def draw_write_strength_logits(key, part):
    order = head_order(key)
    fast = order < HEADS // 2
    blocks = TOKENS // TOK_DEV
    level = jax.random.uniform(jax.random.fold_in(key, 41), (blocks, 1, HEADS), jnp.float32, -5.5, -4.5)
    jiggle = jax.random.uniform(jax.random.fold_in(key, 42), (blocks, TOK_DEV, HEADS), jnp.float32, -1.0, 1.0)
    wide = jax.random.uniform(jax.random.fold_in(key, 43), (blocks, TOK_DEV, HEADS), jnp.float32, -3.0, 3.0)
    picked = jnp.where(fast[None, None, :], wide, level + jiggle)
    return picked.reshape(TOKENS, HEADS).astype(jnp.bfloat16)


def draw_decay_input_logits(key, part):
    shifts = jax.random.uniform(jax.random.fold_in(key, 21), (TOKENS // TOK_DEV, 1, HEADS), jnp.float32, -0.8, 0.8)
    noise = jnp.clip(jax.random.normal(jax.random.fold_in(key, 22), (TOKENS // TOK_DEV, TOK_DEV, HEADS), jnp.float32), -3.5, 3.5)
    return (noise + shifts).reshape(TOKENS, HEADS).astype(jnp.bfloat16)


def draw_extra_log_decay(key, part):
    chance = jax.random.uniform(jax.random.fold_in(key, 31), (TOKENS, HEADS), jnp.float32)
    depth = jax.random.uniform(jax.random.fold_in(key, 32), (TOKENS, HEADS), jnp.float32, 0.22, 0.69)
    return jnp.where(chance < 6.0 / TOKENS, -depth, 0.0).astype(jnp.float32)


def steps_of(stream_key, dims, shards, low, largest):
    def one(dim, blocks):
        draws = jax.random.uniform(jax.random.fold_in(jax.random.fold_in(stream_key, 6), dim), (blocks,), jnp.float32, low / len(shards), largest / len(shards))
        return jnp.repeat(jnp.exp(draws), dims[dim] // blocks).reshape((-1,) + (1,) * (len(dims) - dim - 1))

    level = one(*shards[0])
    for cut in shards[1:]:
        level = level * one(*cut)
    return level


def routed_block(own_key, own, number, rows, count, top, most, slope):
    sequence = jax.random.permutation(own_key, count)
    crowded, ordinary = shares(count, rows * top, most, slope, True), shares(count, rows * top, most, slope, False)
    places = jnp.arange(count)

    def named(lengths, rotation):
        used = int((lengths > 0).sum())
        fixed = max(1, used // 4)
        shifted = fixed + (places - fixed + rotation * (used - fixed)) % max(1, count - fixed)
        return jnp.zeros((count,), jnp.int32).at[sequence[jnp.where(places < fixed, places, shifted)]].set(jnp.asarray(lengths, jnp.int32))

    lengths = jnp.where(number % 4 == 0, named(crowded, number // 4), named(ordinary, number - number // 4 - 1))
    mixed = jax.random.permutation(jax.random.fold_in(own, 3), count)
    giver, taker = mixed[0:count // 2 * 2:2], mixed[1:count // 2 * 2:2]
    slack = jnp.minimum(lengths[giver] - 1, most - lengths[taker]) // 2
    slack = jnp.where((giver == sequence[0]) | (taker == sequence[0]) | (lengths[taker] == 0), 0, jnp.maximum(slack, 0))
    shifted = jax.random.randint(jax.random.fold_in(own, 4), (count // 2,), 0, 1 << 20) % (slack + 1)
    lengths = lengths.at[giver].add(-shifted).at[taker].add(shifted)
    items = jnp.searchsorted(jnp.cumsum(lengths), jnp.arange(rows * top), side="right").astype(jnp.int32)
    grid = items.reshape(top, rows).T
    grid = grid[jax.random.permutation(jax.random.fold_in(own, 1), rows)]
    rotation = jax.random.randint(jax.random.fold_in(own, 2), (rows, 1), 0, top)
    return jnp.take_along_axis(grid, (jnp.arange(top)[None, :] + rotation) % top, axis=1)


def shares(number_of, total, most, lean, full):
    loads = [(1 << 20) // math.isqrt(grade ** lean) + 1 for grade in range(1, number_of + 1)]
    largest = most if full else min(most, max(-(-total // number_of), total * loads[0] // sum(loads)))
    least = 1 if total - largest >= number_of - 1 else 0
    holding, surplus = [largest] + [least] * (number_of - 1), total - largest - least * (number_of - 1)
    while surplus > 0:
        free = [i for i in range(1, number_of) if holding[i] < largest] or [i for i in range(1, number_of) if holding[i] < most]
        whole, remaining = sum([loads[i] for i in free]), surplus
        for i in free:
            addition = min(most - holding[i], max(1, remaining * loads[i] // whole), surplus)
            holding[i] = holding[i] + addition
            surplus = surplus - addition
    return np.array(holding)


def gaussian(stream_key, shape, scale, most, pieces=(), kind=jnp.bfloat16):
    values = jax.random.normal(stream_key, shape, jnp.float32) * scale
    if len(pieces) > 0:
        values = steps_of(stream_key, shape, pieces, -0.22, 0.18) * values
    return jnp.clip(values, min=-most, max=most).astype(kind)


def setup_inputs(seed: int = 0) -> dict:
    splits = jax.random.split(jax.random.key(seed), 21)
    projected_queries = gaussian(splits[0], (TOKENS, HEADS * HD), 1.0, 6.0, ((0, 64), (1, 2)))
    projected_keys = gaussian(splits[1], (TOKENS, HEADS * HD), 1.0, 6.0, ((0, 64), (1, 2)))
    projected_values = gaussian(splits[2], (TOKENS, HEADS * HD), 1.0, 6.0, ((0, 64), (1, 2)))
    output_gate_values = gaussian(splits[3], (TOKENS, HEADS * HD), 1.0, 6.0, ((0, 64), (1, 2)))
    write_strength_logits = draw_write_strength_logits(jax.random.fold_in(splits[20], 71), 0)
    decay_input_logits = draw_decay_input_logits(jax.random.fold_in(splits[20], 71), 0)
    head_rate_logarithm = draw_head_rate_logarithm(jax.random.fold_in(splits[20], 71), 0)
    extra_log_decay = draw_extra_log_decay(jax.random.fold_in(splits[20], 71), 0)
    per_head_norm_gain = jnp.clip(1.0 + 0.18 * jax.random.normal(splits[8], (HD,), jnp.float32), 0.1, 1.9)
    output_matrix = gaussian(splits[9], (HEADS * HD, D), (HEADS * HD) ** -0.5, 0.1875)
    residual = gaussian(splits[10], (TOKENS, D), 1.0, 6.0, ((0, 128),))
    mixture_norm_gain = jnp.clip(1.0 + 0.18 * jax.random.normal(splits[11], (D,), jnp.float32), 0.1, 1.9)
    selected_expert_index_keys = jax.random.split(jax.random.fold_in(splits[12], 1), TOKENS // (TOK_DEV // N_TP))
    selected_expert_index_turns = jax.random.permutation(jax.random.fold_in(splits[12], 3), TOKENS // (TOK_DEV // N_TP))
    selected_expert_index = jax.vmap(lambda own, number: routed_block(jax.random.fold_in(splits[12], 2), own, number, TOK_DEV // N_TP, EXPERTS, TOP_K, CAP, 1))(selected_expert_index_keys, selected_expert_index_turns).reshape((TOKENS, TOP_K))
    routing_weight = jnp.clip(0.1 + 0.79999997 * jax.random.uniform(splits[13], (TOKENS, TOP_K), jnp.float32) ** steps_of(splits[13], (TOKENS, TOP_K), ((0, 128),), -0.2, 0.2), 0.1, 0.9)
    routed_gate_weight = gaussian(splits[14], (EXPERTS, D, EFF), D ** -0.5, 0.125, ((0, 128),))
    routed_up_weight = gaussian(splits[15], (EXPERTS, D, EFF), D ** -0.5, 0.125, ((0, 128),))
    routed_down_weight = gaussian(splits[16], (EXPERTS, EFF, D), EFF ** -0.5, 0.25, ((0, 128),))
    common_gate_weight = gaussian(splits[17], (D, SFF), D ** -0.5, 0.125)
    common_up_weight = gaussian(splits[18], (D, SFF), D ** -0.5, 0.125)
    common_down_weight = gaussian(splits[19], (SFF, D), SFF ** -0.5, 0.25)
    return dict(projected_queries=projected_queries, projected_keys=projected_keys, projected_values=projected_values, output_gate_values=output_gate_values, write_strength_logits=write_strength_logits, decay_input_logits=decay_input_logits, head_rate_logarithm=head_rate_logarithm, extra_log_decay=extra_log_decay, per_head_norm_gain=per_head_norm_gain, output_matrix=output_matrix, residual=residual, mixture_norm_gain=mixture_norm_gain, selected_expert_index=selected_expert_index, routing_weight=routing_weight, routed_gate_weight=routed_gate_weight, routed_up_weight=routed_up_weight, routed_down_weight=routed_down_weight, common_gate_weight=common_gate_weight, common_up_weight=common_up_weight, common_down_weight=common_down_weight)


EPS = 1e-06
HIGH = lax.Precision.HIGHEST

def unit_heads(raw, heads):
    active = jax.nn.silu(raw.astype(jnp.float32)).reshape(raw.shape[0], heads, -1)
    return active * lax.rsqrt(lax.optimization_barrier(jnp.sum(active * active, axis=-1, keepdims=True)) + EPS)

def prepare_inputs(projected_queries, projected_keys, projected_values, write_strength_logits, decay_input_logits, head_rate_logarithm, extra_log_decay):
    heads = head_rate_logarithm.shape[0]
    queries = unit_heads(projected_queries, heads)
    keys = unit_heads(projected_keys, heads)
    values = jax.nn.silu(projected_values.astype(jnp.float32)).reshape(projected_values.shape[0], heads, -1)
    beta = jax.nn.sigmoid(write_strength_logits.astype(jnp.float32))
    decay_logarithm = extra_log_decay - jnp.exp(head_rate_logarithm)[None, :] * jax.nn.softplus(decay_input_logits.astype(jnp.float32) - 6.0)
    return (queries, keys, values, beta, decay_logarithm)

def block_terms(queries, keys, values, beta, decay_logarithm):
    length, heads, width = queries.shape
    number = length // SPAN

    def split(array):
        return jnp.moveaxis(array.reshape(number, SPAN, heads, -1), 2, 0)
    q_blocks = split(queries)
    k_blocks = split(keys)
    v_blocks = split(values)
    b_blocks = split(beta[..., None])[..., 0]
    g_cumul = jnp.cumsum(split(decay_logarithm[..., None])[..., 0], axis=-1)
    place = jnp.arange(SPAN)
    causal = place[:, None] >= place[None, :]
    strict = place[:, None] > place[None, :]
    spread = jnp.where(causal, g_cumul[..., :, None] - g_cumul[..., None, :], 0.0)
    decay = jnp.where(causal, jnp.exp(spread), 0.0)
    k_beta = k_blocks * b_blocks[..., None]
    inner = jnp.einsum('hncd,hnsd->hncs', k_beta, k_blocks, precision=HIGH)
    lower = jnp.where(strict, inner * decay, 0.0) + jnp.eye(SPAN, dtype=jnp.float32)
    right = jnp.concatenate([v_blocks * b_blocks[..., None], k_beta * jnp.exp(g_cumul)[..., None]], axis=-1)
    solved = jax.scipy.linalg.solve_triangular(lower, right, lower=True, unit_diagonal=True)
    u_part = solved[..., :width]
    w_part = solved[..., width:]
    scores = jnp.einsum('hncd,hnsd->hncs', q_blocks, k_blocks, precision=HIGH) * decay
    q_decayed = q_blocks * jnp.exp(g_cumul)[..., None]
    log_last = g_cumul[..., -1]
    k_decayed = k_blocks * jnp.exp(log_last[..., None] - g_cumul)[..., None]
    return (q_decayed, scores, u_part, w_part, k_decayed, log_last)

def run_blocks(terms, start):

    def advance(state, items):
        q_one, s_one, u_one, w_one, k_one, log_one = items
        fresh = u_one - jnp.einsum('hcd,hde->hce', w_one, state, precision=HIGH)
        result = jnp.einsum('hcd,hde->hce', q_one, state, precision=HIGH)
        result = result + jnp.einsum('hcs,hse->hce', s_one, fresh, precision=HIGH)
        state = state * jnp.exp(log_one)[:, None, None] + jnp.einsum('hcd,hce->hde', k_one, fresh, precision=HIGH)
        return (state, result)
    items = tuple((jnp.moveaxis(array, 1, 0) for array in terms))
    _, results = lax.scan(advance, start, items)
    number, heads, span, width = results.shape
    return results.transpose(0, 2, 1, 3).reshape(number * span, heads, width)

def finish(head_mix, output_gate_values, per_head_norm_gain):
    length, heads, width = head_mix.shape
    scaled = head_mix * lax.rsqrt(lax.optimization_barrier(jnp.mean(head_mix * head_mix, axis=-1, keepdims=True)) + EPS)
    gated = scaled * per_head_norm_gain * jax.nn.silu(output_gate_values.astype(jnp.float32).reshape(length, heads, width))
    return gated.reshape(length, heads * width).astype(jnp.bfloat16)

def normalize(stream, gain):
    wide = stream.astype(jnp.float32)
    return (wide * lax.rsqrt(lax.optimization_barrier(jnp.mean(wide * wide, axis=-1, keepdims=True)) + EPS) * gain).astype(jnp.bfloat16)

def feed_forward(rows, w_gate, w_up, w_down):
    hidden = jax.nn.silu(jnp.dot(rows.astype(jnp.float32), w_gate.astype(jnp.float32), preferred_element_type=jnp.float32))
    hidden = (hidden * jnp.dot(rows.astype(jnp.float32), w_up.astype(jnp.float32), preferred_element_type=jnp.float32)).astype(jnp.bfloat16)
    return jnp.dot(hidden.astype(jnp.float32), w_down.astype(jnp.float32), preferred_element_type=jnp.float32)

def routed_sum(normed, selected_expert_index, routing_weight, routed_gate_weight, routed_up_weight, routed_down_weight):
    length = normed.shape[0]
    room = N_SP * N_TP * CAP
    flat_ids = selected_expert_index.reshape(-1)
    flat_rows = (jnp.arange(flat_ids.shape[0]) // TOP_K).astype(jnp.int32)
    flat_weight = routing_weight.reshape(-1)

    def one_expert(total, items):
        w_gate, w_up, w_down, expert = items
        chosen = flat_ids == expert
        slot = (jnp.cumsum(chosen.astype(jnp.int32)) - 1).astype(jnp.int32)
        target = jnp.where(chosen, slot, room).astype(jnp.int32)
        source = jnp.zeros((room,), jnp.int32).at[target].set(flat_rows, mode='drop')
        weight = jnp.zeros((room,), jnp.float32).at[target].set(flat_weight, mode='drop')
        result = feed_forward(normed[source], w_gate, w_up, w_down).astype(jnp.bfloat16)
        return (total.at[source].add(result.astype(jnp.float32) * weight[:, None]), None)
    experts_all = jnp.arange(EXPERTS).astype(jnp.int32)
    total, _ = lax.scan(one_expert, jnp.zeros((length, D), jnp.float32), (routed_gate_weight, routed_up_weight, routed_down_weight, experts_all))
    return total

def reference(projected_queries, projected_keys, projected_values, output_gate_values, write_strength_logits, decay_input_logits, head_rate_logarithm, extra_log_decay, per_head_norm_gain, output_matrix, residual, mixture_norm_gain, selected_expert_index, routing_weight, routed_gate_weight, routed_up_weight, routed_down_weight, common_gate_weight, common_up_weight, common_down_weight):
    prepared_inputs = prepare_inputs(projected_queries, projected_keys, projected_values, write_strength_logits, decay_input_logits, head_rate_logarithm, extra_log_decay)
    terms = block_terms(*prepared_inputs)
    start = jnp.zeros((HEADS, HD, HD), jnp.float32)
    heads_out = finish(run_blocks(terms, start), output_gate_values, per_head_norm_gain)
    attended = residual.astype(jnp.float32) + jnp.dot(heads_out.astype(jnp.float32), output_matrix.astype(jnp.float32), preferred_element_type=jnp.float32)
    attended = attended.astype(jnp.bfloat16)
    normed = normalize(attended, mixture_norm_gain)
    shared = feed_forward(normed, common_gate_weight, common_up_weight, common_down_weight)
    routed = routed_sum(normed, selected_expert_index, routing_weight, routed_gate_weight, routed_up_weight, routed_down_weight)
    return (attended.astype(jnp.float32) + shared + routed).astype(jnp.bfloat16)
```

```python
import jax
import jax.numpy as jnp
from jax import lax
from jax.experimental import pallas as pl
from jax.experimental.pallas import tpu as pltpu
from jax.sharding import Mesh
from jax.sharding import PartitionSpec as P

TOP_K = 4
HD = 128
BLOCK = 128
KEEP = 8
SP = ("sp_0", "sp_1", "sp_2")
SP_TP = ("sp_0", "sp_1", "sp_2", "tp")
EPS = 1e-06
F32 = jnp.float32
BF16 = jnp.bfloat16


def dot_nn(a, b):
    return lax.dot_general(a, b, (((1,), (0,)), ((), ())), preferred_element_type=F32)


def dot_nt(a, b):
    return lax.dot_general(a, b, (((1,), (1,)), ((), ())), preferred_element_type=F32)


def dot_tn(a, b):
    return lax.dot_general(a, b, (((0,), (0,)), ((), ())), preferred_element_type=F32)


def parts(x):
    high = x.astype(BF16)
    return high, (x - high.astype(F32)).astype(BF16)


def rows_of(*arrays):
    return jnp.concatenate(arrays, axis=0)


def cols_of(*arrays):
    return jnp.concatenate(arrays, axis=1)


def fine(a, b):
    ah, al = a
    bh, bl = b
    return dot_nn(cols_of(ah, al), rows_of(bh, bh)) + dot_nn(ah, bl)


def fine_square(a, b):
    ah, al = a
    bh, bl = b
    both = dot_nn(cols_of(ah, al), rows_of(cols_of(bh, bl), cols_of(bh, jnp.zeros_like(bl))))
    return both[:, :HD] + both[:, HD:]


def sub(pair, rows):
    return pair[0][rows], pair[1][rows]


def terms_kernel(q_ref, k_ref, v_ref, ldb_ref, mb_ref, qe_ref, o0_ref):
    length = q_ref.shape[0]
    number = length // BLOCK
    rows = ldb_ref[0]
    lane = lax.broadcasted_iota(jnp.int32, rows.shape, 1)
    total = rows
    shift = 1
    while shift < length:
        total = total + jnp.where(lane >= shift, pltpu.roll(total, shift, 1), 0.0)
        shift *= 2
    g_row = total[0:1, :]
    g_col = jnp.broadcast_to(g_row, (HD, length)).T
    b_col = jnp.broadcast_to(rows[1:2, :], (HD, length)).T

    def unit(ref):
        x = ref[...].astype(F32)
        active = x * jax.nn.sigmoid(x)
        return active * lax.rsqrt(jnp.sum(active * active, axis=-1, keepdims=True) + EPS)

    queries = unit(q_ref)
    keys = unit(k_ref)
    raw = v_ref[...].astype(F32)
    values = raw * jax.nn.sigmoid(raw)
    grown = jnp.exp(g_col)
    k_beta = keys * b_col
    right = cols_of(k_beta * grown, values * b_col)
    g_last = g_col[length - 1 : length, :]
    k_late = parts(keys * jnp.exp(g_last - g_col))
    qs, ks, kbs = parts(queries), parts(keys), parts(k_beta)
    ii = lax.broadcasted_iota(jnp.int32, (BLOCK, BLOCK), 0)
    jj = lax.broadcasted_iota(jnp.int32, (BLOCK, BLOCK), 1)
    lower, mixing, solved = [], [], []
    for r in range(number):
        here = slice(r * BLOCK, (r + 1) * BLOCK)
        upto = slice(0, (r + 1) * BLOCK)
        left = rows_of(cols_of(kbs[0][here], kbs[1][here]), cols_of(qs[0][here], qs[1][here]))
        high = ks[0][upto]
        both = dot_nt(left, cols_of(high, high)) + dot_nt(rows_of(kbs[0][here], qs[0][here]), ks[1][upto])
        a_row, p_row = [], []
        for c in range(r + 1):
            there = slice(c * BLOCK, (c + 1) * BLOCK)
            gap = g_col[here] - g_row[:, there]
            if c == r:
                gap = jnp.where(ii >= jj, gap, -1e30)
            fade = jnp.exp(gap)
            a_one = both[:BLOCK, there] * fade
            if c == r:
                a_one = jnp.where(ii > jj, a_one, 0.0)
            a_row.append(a_one)
            p_row.append(both[BLOCK:, there] * fade)
        lower.append(a_row)
        mixing.append(p_row)
    eye = (ii == jj).astype(F32)
    inverse = [eye - jnp.where((ii // 2 == jj // 2) & (ii > jj), lower[r][r], 0.0) for r in range(number)]
    size = 2
    while size < BLOCK:
        chosen = (ii // (2 * size) == jj // (2 * size)) & (ii // size > jj // size)
        halves = [parts(t) for t in inverse]
        steps = [
            fine_square(halves[r], parts(jnp.where(chosen, lower[r][r], 0.0))) for r in range(number)
        ]
        inverse = [inverse[r] - fine_square(parts(steps[r]), halves[r]) for r in range(number)]
        size *= 2
    highs, lows = [], []
    for r in range(number):
        here = slice(r * BLOCK, (r + 1) * BLOCK)
        rest = right[here]
        if r > 0:
            known = (rows_of(*highs), rows_of(*lows))
            rest = rest - fine(parts(cols_of(*lower[r][:r])), known)
        one = parts(fine(parts(inverse[r]), parts(rest)))
        highs.append(one[0])
        lows.append(one[1])
        known = (rows_of(*highs), rows_of(*lows))
        mixed = fine(parts(cols_of(*mixing[r])), known)
        qe_ref[here, :] = queries[here] * grown[here] - mixed[:, :HD]
        o0_ref[here, :] = mixed[:, HD:]
    known = (rows_of(*highs), rows_of(*lows))
    moved = dot_tn(rows_of(*k_late), rows_of(known[0], known[0])) + dot_tn(k_late[0], known[1])
    mb_ref[0, :, :HD] = eye * jnp.exp(g_last) - moved[:, :HD]
    mb_ref[0, :, HD:] = moved[:, HD:]


def block_terms(queries, keys, values, log_decay, beta):
    length, wide = queries.shape
    heads = wide // HD
    pad = jnp.zeros((heads, 6, length), F32)
    table = jnp.concatenate([log_decay.T[:, None, :], beta.T[:, None, :], pad], axis=1)
    column = pl.BlockSpec((length, HD), lambda h: (0, h))
    return pl.pallas_call(
        terms_kernel,
        grid=(heads,),
        in_specs=[column, column, column, pl.BlockSpec((1, 8, length), lambda h: (h, 0, 0))],
        out_specs=[pl.BlockSpec((1, HD, 2 * HD), lambda h: (h, 0, 0)), column, column],
        out_shape=[
            jax.ShapeDtypeStruct((heads, HD, 2 * HD), F32),
            jax.ShapeDtypeStruct((length, wide), F32),
            jax.ShapeDtypeStruct((length, wide), F32),
        ],
        name="terms",
    )(queries, keys, values, table)


def shift_in(later):
    wide = lax.broadcasted_iota(jnp.int32, later.shape, 1)
    return jnp.where(wide >= HD, later, 0.0)


def then(later, earlier):
    return fine(parts(later[:, :HD]), parts(earlier)) + shift_in(later)


def identity_map():
    ii = lax.broadcasted_iota(jnp.int32, (HD, 2 * HD), 0)
    jj = lax.broadcasted_iota(jnp.int32, (HD, 2 * HD), 1)
    return (ii == jj).astype(F32)


def all_before_kernel(x_ref, before_ref, total_ref):
    running = identity_map()
    for k in range(x_ref.shape[0]):
        before_ref[k] = running
        running = x_ref[k] if k == 0 else then(x_ref[k], running)
    total_ref[...] = running


def all_before(maps):
    return pl.pallas_call(
        all_before_kernel,
        out_shape=[
            jax.ShapeDtypeStruct(maps.shape, F32),
            jax.ShapeDtypeStruct(maps.shape[1:], F32),
        ],
        name="all_before",
    )(maps)


def mine_before_kernel(mine_ref, x_ref, before_ref, total_ref):
    mine = mine_ref[0]
    running = identity_map()
    before_ref[...] = running
    for k in range(x_ref.shape[0]):
        running = x_ref[k] if k == 0 else then(x_ref[k], running)

        @pl.when(mine == k + 1)
        def _(running=running):
            before_ref[...] = running

    total_ref[...] = running


def mine_before(maps, mine):
    one = jax.ShapeDtypeStruct(maps.shape[1:], F32)
    return pl.pallas_call(
        mine_before_kernel,
        in_specs=[
            pl.BlockSpec(memory_space=pltpu.SMEM),
            pl.BlockSpec(memory_space=pltpu.VMEM),
        ],
        out_shape=[one, one],
        name="mine_before",
    )(mine, maps)


def states_kernel(mine_ref, outer_ref, middle_ref, inner_ref, out_ref, state_ref):
    mine = mine_ref[0]
    state_ref[...] = jnp.zeros_like(state_ref)
    for k in range(outer_ref.shape[0] - 1):

        @pl.when(mine > k)
        def _(k=k):
            state_ref[...] = (
                fine(parts(outer_ref[k, :, :HD]), parts(state_ref[...])) + outer_ref[k, :, HD:]
            )

    state = fine(parts(middle_ref[:, :HD]), parts(state_ref[...])) + middle_ref[:, HD:]
    pair = parts(state)
    out_ref[0] = state
    for k in range(1, inner_ref.shape[0]):
        out_ref[k] = fine(parts(inner_ref[k, :, :HD]), pair) + inner_ref[k, :, HD:]


def states(outer, mine, middle, inner):
    return pl.pallas_call(
        states_kernel,
        in_specs=[pl.BlockSpec(memory_space=pltpu.SMEM)]
        + [pl.BlockSpec(memory_space=pltpu.VMEM)] * 3,
        out_shape=jax.ShapeDtypeStruct((inner.shape[0], HD, HD), F32),
        scratch_shapes=[pltpu.VMEM((HD, HD), F32)],
        name="states",
    )(mine, outer, middle, inner)


def entering(maps):
    by_position = lax.all_to_all(maps, "sp_2", split_axis=0, concat_axis=0, tiled=True)
    inner, line = all_before(by_position)
    lines = lax.all_gather(line, "sp_1")
    middle, plane = mine_before(lines, lax.axis_index("sp_1").reshape(1).astype(jnp.int32))
    planes = lax.all_gather(plane, "sp_0")
    found = states(planes, lax.axis_index("sp_0").reshape(1).astype(jnp.int32), middle, inner)
    return lax.all_to_all(found, "sp_2", split_axis=0, concat_axis=0, tiled=True)


def finish_kernel(qe_ref, o0_ref, s_ref, gate_ref, gain_ref, out_ref):
    mix = o0_ref[...] + fine(parts(qe_ref[...]), parts(s_ref[0]))
    scaled = mix * lax.rsqrt(jnp.mean(mix * mix, axis=-1, keepdims=True) + EPS)
    gate = gate_ref[...].astype(F32)
    out_ref[...] = (scaled * gain_ref[...] * (gate * jax.nn.sigmoid(gate))).astype(BF16)


def finish(qe, o0, state, gate, gain):
    length, wide = qe.shape
    column = pl.BlockSpec((length, HD), lambda h: (0, h))
    return pl.pallas_call(
        finish_kernel,
        grid=(wide // HD,),
        in_specs=[
            column,
            column,
            pl.BlockSpec((1, HD, HD), lambda h: (h, 0, 0)),
            column,
            pl.BlockSpec((1, HD), lambda h: (0, 0)),
        ],
        out_specs=column,
        out_shape=jax.ShapeDtypeStruct((length, wide), BF16),
        name="finish",
    )(qe, o0, state, gate, gain.reshape(1, HD))


def normalize(wide, gain):
    return (wide * lax.rsqrt(jnp.mean(wide * wide, axis=-1, keepdims=True) + EPS) * gain).astype(
        BF16
    )


def feed_forward(rows, w_gate, w_up, w_down):
    hidden = jax.nn.silu(jnp.dot(rows, w_gate, preferred_element_type=F32))
    hidden = (hidden * jnp.dot(rows, w_up, preferred_element_type=F32)).astype(BF16)
    return jnp.dot(hidden, w_down, preferred_element_type=F32)


def exchange(rows):
    return lax.all_to_all(rows, SP_TP, split_axis=0, concat_axis=0, tiled=True)


def routes(index, weight, experts, room):
    length = index.shape[0]
    ids = jnp.arange(experts, dtype=jnp.int32)[:, None]
    named = jnp.zeros((experts, length), F32)
    weights = jnp.zeros((experts, length), F32)
    for j in range(index.shape[1]):
        here = index[:, j][None, :] == ids
        named = named + here.astype(F32)
        weights = weights + jnp.where(here, weight[:, j][None, :], 0.0)
    place = jnp.arange(length, dtype=jnp.int32)
    earlier = (place[:, None] < place[None, :]).astype(BF16)
    slot = jnp.dot(named.astype(BF16), earlier, preferred_element_type=F32)
    slot = jnp.where(named > 0, slot, -1.0)[:, None, :]
    step = jnp.arange(KEEP, dtype=jnp.int32)[None, :, None]
    extra = room - KEEP
    first = slot == step.astype(F32)
    rest = slot == (KEEP + step % extra).astype(F32)
    lead = rest & (step < extra)
    tail = rest & (step >= extra)
    weights = weights[:, None, :]

    def flat(mask):
        return mask.reshape(experts * KEEP, length)

    out = [flat(m.astype(BF16)) for m in (first, lead, tail)]
    back = [flat(jnp.where(m, weights, 0.0).astype(BF16)) for m in (first, lead, tail)]
    return out, back


def shards(
    projected_queries,
    projected_keys,
    projected_values,
    output_gate_values,
    write_strength_logits,
    decay_input_logits,
    head_rate_logarithm,
    extra_log_decay,
    per_head_norm_gain,
    output_matrix,
    residual,
    mixture_norm_gain,
    selected_expert_index,
    routing_weight,
    routed_gate_weight,
    routed_up_weight,
    routed_down_weight,
    common_gate_weight,
    common_up_weight,
    common_down_weight,
):
    beta = jax.nn.sigmoid(write_strength_logits.astype(F32))
    log_decay = extra_log_decay - jnp.exp(head_rate_logarithm)[None, :] * jax.nn.softplus(
        decay_input_logits.astype(F32) - 6.0
    )
    maps, qe, o0 = block_terms(projected_queries, projected_keys, projected_values, log_decay, beta)
    state = entering(maps)
    heads_out = finish(qe, o0, state, output_gate_values, per_head_norm_gain)
    length = residual.shape[0]
    wide = heads_out.shape[1]
    pieces = lax.all_to_all(
        heads_out.reshape(2, length, wide), "tp", split_axis=0, concat_axis=0, tiled=True
    )
    projected = jnp.dot(pieces[0], output_matrix[:wide], preferred_element_type=F32) + jnp.dot(
        pieces[1], output_matrix[wide:], preferred_element_type=F32
    )
    attended = (residual.astype(F32) + projected).astype(BF16)
    normed = normalize(attended.astype(F32), mixture_norm_gain)

    experts = lax.axis_size(SP) * lax.axis_size("tp")
    room = max(2, length * TOP_K * 3 // (2 * experts))
    extra = room - KEEP
    dim = normed.shape[1]
    half = dim // 2
    (first, lead, tail), (w_first, w_lead, w_tail) = routes(
        selected_expert_index, routing_weight, experts, room
    )
    main_out = jnp.dot(first, normed, preferred_element_type=F32).astype(BF16)
    rest_out = (
        jnp.dot(lead, normed[:, :half], preferred_element_type=F32)
        + jnp.dot(tail, normed[:, half:], preferred_element_type=F32)
    ).astype(BF16)
    main_in = exchange(main_out.reshape(experts, KEEP, dim))
    rest_in = exchange(rest_out.reshape(experts, KEEP, half))
    shared = feed_forward(normed, common_gate_weight, common_up_weight, common_down_weight)

    weights = (routed_gate_weight[0], routed_up_weight[0], routed_down_weight[0])
    main_rows = feed_forward(main_in.reshape(experts * KEEP, dim), *weights).astype(BF16)
    main_back = exchange(main_rows.reshape(experts, KEEP, dim)).reshape(experts * KEEP, dim)
    unfolded = rest_in.reshape(experts, 2, extra, half).transpose(0, 2, 1, 3)
    rest_rows = feed_forward(unfolded.reshape(experts * extra, dim), *weights).astype(BF16)
    folded = rest_rows.reshape(experts, extra, 2, half).transpose(0, 2, 1, 3)
    rest_back = exchange(folded.reshape(experts, KEEP, half)).reshape(experts * KEEP, half)

    def combine(table, rows):
        return lax.dot_general(table, rows, (((0,), (0,)), ((), ())), preferred_element_type=F32)

    routed = combine(w_first, main_back) + jnp.concatenate(
        [combine(w_lead, rest_back), combine(w_tail, rest_back)], axis=1
    )
    return (attended.astype(F32) + shared + routed).astype(BF16)


def solution(mesh):
    finer = Mesh(mesh.devices.reshape(4, 4, 4, mesh.shape["tp"]), ("sp_0", "sp_1", "sp_2", "tp"))
    in_specs = (
        P(SP, "tp"),
        P(SP, "tp"),
        P(SP, "tp"),
        P(SP, "tp"),
        P(SP, "tp"),
        P(SP, "tp"),
        P("tp"),
        P(SP, "tp"),
        P(),
        P(),
        P(SP_TP, None),
        P(),
        P(SP_TP, None),
        P(SP_TP, None),
        P(SP_TP, None, None),
        P(SP_TP, None, None),
        P(SP_TP, None, None),
        P(),
        P(),
        P(),
    )
    out_specs = P(SP_TP, None)
    return jax.shard_map(
        shards, mesh=finer, in_specs=in_specs, out_specs=out_specs, check_vma=False
    )
```

```python
import jax
import jax.numpy as jnp
from jax import lax
from jax.experimental import pallas as pl
from jax.experimental.pallas import tpu as pltpu
from jax.sharding import Mesh
from jax.sharding import PartitionSpec as P

TOP_K = 4
HD = 128
BLOCK = 128
KEEP = 8
SP = ("sp_0", "sp_1", "sp_2")
SP_TP = ("sp_0", "sp_1", "sp_2", "tp")
EPS = 1e-06
F32 = jnp.float32
BF16 = jnp.bfloat16


def dot_nn(a, b):
    return lax.dot_general(a, b, (((1,), (0,)), ((), ())), preferred_element_type=F32)


def dot_nt(a, b):
    return lax.dot_general(a, b, (((1,), (1,)), ((), ())), preferred_element_type=F32)


def dot_tn(a, b):
    return lax.dot_general(a, b, (((0,), (0,)), ((), ())), preferred_element_type=F32)


def parts(x):
    high = x.astype(BF16)
    return high, (x - high.astype(F32)).astype(BF16)


def rows_of(*arrays):
    return jnp.concatenate(arrays, axis=0)


def cols_of(*arrays):
    return jnp.concatenate(arrays, axis=1)


def fine(a, b):
    ah, al = a
    bh, bl = b
    return dot_nn(cols_of(ah, al), rows_of(bh, bh)) + dot_nn(ah, bl)


def fine_square(a, b):
    ah, al = a
    bh, bl = b
    both = dot_nn(cols_of(ah, al), rows_of(cols_of(bh, bl), cols_of(bh, jnp.zeros_like(bl))))
    return both[:, :HD] + both[:, HD:]


def sub(pair, rows):
    return pair[0][rows], pair[1][rows]


def terms_kernel(
    place_ref, rate_ref, q_ref, k_ref, v_ref, write_ref, decay_ref, extra_ref, *out_refs
):
    map_refs, (qe_ref, o0_ref) = out_refs[:-2], out_refs[-2:]
    length = q_ref.shape[0]
    number = length // BLOCK
    head = pl.program_id(0)
    slot = (head + len(map_refs) - place_ref[0]) % len(map_refs)

    def own(ref):
        table = ref[...].astype(F32)
        which = lax.broadcasted_iota(jnp.int32, table.shape, 0)
        return jnp.sum(jnp.where(which == head, table, 0.0), axis=0, keepdims=True)

    raw_decay = own(decay_ref) - 6.0
    soft = jnp.maximum(raw_decay, 0.0) + jnp.log1p(jnp.exp(-jnp.abs(raw_decay)))
    rate = jnp.exp(jnp.full((1, length), rate_ref[head], F32))
    log_decay = own(extra_ref) - rate * soft
    beta_row = jax.nn.sigmoid(own(write_ref))
    rows = jnp.broadcast_to(log_decay, (8, length))
    lane = lax.broadcasted_iota(jnp.int32, rows.shape, 1)
    total = rows
    shift = 1
    while shift < length:
        total = total + jnp.where(lane >= shift, pltpu.roll(total, shift, 1), 0.0)
        shift *= 2
    g_row = total[0:1, :]
    g_col = jnp.broadcast_to(g_row, (HD, length)).T
    b_col = jnp.broadcast_to(beta_row, (HD, length)).T

    def unit(ref):
        x = ref[...].astype(F32)
        active = x * jax.nn.sigmoid(x)
        return active * lax.rsqrt(jnp.sum(active * active, axis=-1, keepdims=True) + EPS)

    queries = unit(q_ref)
    keys = unit(k_ref)
    raw = v_ref[...].astype(F32)
    values = raw * jax.nn.sigmoid(raw)
    grown = jnp.exp(g_col)
    k_beta = keys * b_col
    right = cols_of(k_beta * grown, values * b_col)
    g_last = g_col[length - 1 : length, :]
    k_late = parts(keys * jnp.exp(g_last - g_col))
    qs, ks, kbs = parts(queries), parts(keys), parts(k_beta)
    ii = lax.broadcasted_iota(jnp.int32, (BLOCK, BLOCK), 0)
    jj = lax.broadcasted_iota(jnp.int32, (BLOCK, BLOCK), 1)
    lower, mixing, solved = [], [], []
    for r in range(number):
        here = slice(r * BLOCK, (r + 1) * BLOCK)
        upto = slice(0, (r + 1) * BLOCK)
        left = rows_of(cols_of(kbs[0][here], kbs[1][here]), cols_of(qs[0][here], qs[1][here]))
        high = ks[0][upto]
        both = dot_nt(left, cols_of(high, high)) + dot_nt(rows_of(kbs[0][here], qs[0][here]), ks[1][upto])
        a_row, p_row = [], []
        for c in range(r + 1):
            there = slice(c * BLOCK, (c + 1) * BLOCK)
            gap = g_col[here] - g_row[:, there]
            if c == r:
                gap = jnp.where(ii >= jj, gap, -1e30)
            fade = jnp.exp(gap)
            a_one = both[:BLOCK, there] * fade
            if c == r:
                a_one = jnp.where(ii > jj, a_one, 0.0)
            a_row.append(a_one)
            p_row.append(both[BLOCK:, there] * fade)
        lower.append(a_row)
        mixing.append(p_row)
    eye = (ii == jj).astype(F32)
    inverse = [eye - jnp.where((ii // 2 == jj // 2) & (ii > jj), lower[r][r], 0.0) for r in range(number)]
    size = 2
    while size < BLOCK:
        chosen = (ii // (2 * size) == jj // (2 * size)) & (ii // size > jj // size)
        halves = [parts(t) for t in inverse]
        steps = [
            fine_square(halves[r], parts(jnp.where(chosen, lower[r][r], 0.0))) for r in range(number)
        ]
        inverse = [inverse[r] - fine_square(parts(steps[r]), halves[r]) for r in range(number)]
        size *= 2
    highs, lows = [], []
    for r in range(number):
        here = slice(r * BLOCK, (r + 1) * BLOCK)
        rest = right[here]
        if r > 0:
            known = (rows_of(*highs), rows_of(*lows))
            rest = rest - fine(parts(cols_of(*lower[r][:r])), known)
        one = parts(fine(parts(inverse[r]), parts(rest)))
        highs.append(one[0])
        lows.append(one[1])
        known = (rows_of(*highs), rows_of(*lows))
        mixed = fine(parts(cols_of(*mixing[r])), known)
        qe_ref[here, :] = queries[here] * grown[here] - mixed[:, :HD]
        o0_ref[here, :] = mixed[:, HD:]
    known = (rows_of(*highs), rows_of(*lows))
    moved = dot_tn(rows_of(*k_late), rows_of(known[0], known[0])) + dot_tn(k_late[0], known[1])
    whole = cols_of(eye * jnp.exp(g_last) - moved[:, :HD], moved[:, HD:])
    for s, map_ref in enumerate(map_refs):

        @pl.when(slot == s)
        def _(map_ref=map_ref):
            map_ref[...] = whole


def block_terms(queries, keys, values, write_logits, decay_logits, rates, extra, place):
    length, wide = queries.shape
    heads = wide // HD
    column = pl.BlockSpec((length, HD), lambda h: (0, h))
    table = pl.BlockSpec((heads, length), lambda h: (0, 0))
    small = pl.BlockSpec(memory_space=pltpu.SMEM)
    one_map = pl.BlockSpec((HD, 2 * HD), lambda h: (0, 0))
    out = pl.pallas_call(
        terms_kernel,
        grid=(heads,),
        in_specs=[small, small, column, column, column, table, table, table],
        out_specs=[one_map] * heads + [column, column],
        out_shape=[jax.ShapeDtypeStruct((HD, 2 * HD), F32)] * heads
        + [jax.ShapeDtypeStruct((length, wide), F32)] * 2,
        name="terms",
    )(place, rates, queries, keys, values, write_logits.T, decay_logits.T, extra.T)
    return out[:heads], out[heads], out[heads + 1]


def shift_in(later):
    wide = lax.broadcasted_iota(jnp.int32, later.shape, 1)
    return jnp.where(wide >= HD, later, 0.0)


def then(later, earlier):
    return fine(parts(later[:, :HD]), parts(earlier)) + shift_in(later)


def identity_map():
    ii = lax.broadcasted_iota(jnp.int32, (HD, 2 * HD), 0)
    jj = lax.broadcasted_iota(jnp.int32, (HD, 2 * HD), 1)
    return (ii == jj).astype(F32)


def in_order(place, refs, held_ref):
    number = len(refs)
    for s, ref in enumerate(refs):
        held_ref[(place + number - s) % number] = ref[...]


def all_before_kernel(place_ref, *refs):
    maps, (before_ref, total_ref, held_ref) = refs[:-3], refs[-3:]
    in_order(place_ref[0], maps, held_ref)
    running = identity_map()
    for k in range(len(maps)):
        before_ref[k] = running
        running = held_ref[k] if k == 0 else then(held_ref[k], running)
    total_ref[...] = running


def mine_before_kernel(place_ref, *refs):
    maps, (before_ref, total_ref, held_ref) = refs[:-3], refs[-3:]
    place = place_ref[0]
    in_order(place, maps, held_ref)
    running = identity_map()
    before_ref[...] = running
    for k in range(len(maps)):
        running = held_ref[k] if k == 0 else then(held_ref[k], running)

        @pl.when(place == k + 1)
        def _(running=running):
            before_ref[...] = running

    total_ref[...] = running


def small_call(kernel, name, out_shape, scratch, place, *arrays):
    return pl.pallas_call(
        kernel,
        in_specs=[pl.BlockSpec(memory_space=pltpu.SMEM)]
        + [pl.BlockSpec(memory_space=pltpu.VMEM)] * len(arrays),
        out_shape=out_shape,
        scratch_shapes=scratch,
        name=name,
    )(place, *arrays)


def states_kernel(place_ref, one_ref, two_ref, three_ref, middle_ref, inner_ref, *out_refs):
    state = three_ref[:, HD:]
    for ref in (two_ref, one_ref, middle_ref):
        state = fine(parts(ref[:, :HD]), parts(state)) + ref[:, HD:]
    pair = parts(state)
    number = len(out_refs)
    for s, out_ref in enumerate(out_refs):
        k = (place_ref[0] + number - s) % number
        out_ref[...] = fine(parts(inner_ref[k, :, :HD]), pair) + inner_ref[k, :, HD:]


def ring(array, axis, step):
    count = lax.axis_size(axis)
    return lax.ppermute(array, axis, [(i, (i + step) % count) for i in range(count)])


def onward(array, axis, step):
    count = lax.axis_size(axis)
    return lax.ppermute(array, axis, [(i, i + step) for i in range(count - step)])


def place_on(axis):
    return lax.axis_index(axis).reshape(1).astype(jnp.int32)


def entering(maps, place):
    number = len(maps)
    one = jax.ShapeDtypeStruct(maps[0].shape, F32)
    many = jax.ShapeDtypeStruct((number,) + maps[0].shape, F32)
    held = [pltpu.VMEM((number,) + maps[0].shape, F32)]
    arrived = [maps[0]] + [ring(maps[s], "sp_2", s) for s in (2, 1, 3)]
    arrived = [arrived[0], arrived[2], arrived[1], arrived[3]]
    inner, line = small_call(all_before_kernel, "all_before", [many, one], held, place, *arrived)
    two, first, three = [ring(line, "sp_1", s) for s in (2, 1, 3)]
    middle, plane = small_call(
        mine_before_kernel, "mine_before", [one, one], held, place_on("sp_1"), line, first, two, three
    )
    two, first, three = [onward(plane, "sp_0", s) for s in (2, 1, 3)]
    found = small_call(
        states_kernel,
        "states",
        [jax.ShapeDtypeStruct((HD, HD), F32)] * number,
        (),
        place,
        first,
        two,
        three,
        middle,
        inner,
    )
    two, first, three = [ring(found[s], "sp_2", number - s) for s in (2, 1, 3)]
    return [found[0], first, two, three]


def finish_kernel(place_ref, core_ref, qe_ref, o0_ref, gate_ref, gain_ref, *refs):
    states, (keep_ref, send_ref, whole_ref) = refs[:-3], refs[-3:]
    number = len(states)
    slot = (pl.program_id(0) + number - place_ref[0]) % number
    state = states[0][...]
    for s in range(1, number):
        state = jnp.where(slot == s, states[s][...], state)
    mix = o0_ref[...] + fine(parts(qe_ref[...]), parts(state))
    scaled = mix * lax.rsqrt(jnp.mean(mix * mix, axis=-1, keepdims=True) + EPS)
    gate = gate_ref[...].astype(F32)
    whole_ref[...] = scaled * gain_ref[...] * (gate * jax.nn.sigmoid(gate))
    half = keep_ref.shape[0]
    core = core_ref[0]
    keep_ref[...] = whole_ref[pl.ds(core * half, half), :].astype(BF16)
    send_ref[...] = whole_ref[pl.ds((1 - core) * half, half), :].astype(BF16)


def finish(qe, o0, states, gate, gain, place):
    length, wide = qe.shape
    column = pl.BlockSpec((length, HD), lambda h: (0, h))
    half = pl.BlockSpec((length // 2, HD), lambda h: (0, h))
    small = pl.BlockSpec(memory_space=pltpu.SMEM)
    one = pl.BlockSpec((HD, HD), lambda h: (0, 0))
    return pl.pallas_call(
        finish_kernel,
        grid=(wide // HD,),
        in_specs=[small, small, column, column, column, pl.BlockSpec((1, HD), lambda h: (0, 0))]
        + [one] * len(states),
        out_specs=[half, half],
        out_shape=[jax.ShapeDtypeStruct((length // 2, wide), BF16)] * 2,
        scratch_shapes=[pltpu.VMEM((length, HD), F32)],
        name="finish",
    )(place, place_on("tp"), qe, o0, gate, gain.reshape(1, HD), *states)


def normalize(wide, gain):
    return (wide * lax.rsqrt(jnp.mean(wide * wide, axis=-1, keepdims=True) + EPS) * gain).astype(
        BF16
    )


def feed_forward(rows, w_gate, w_up, w_down):
    hidden = jax.nn.silu(jnp.dot(rows, w_gate, preferred_element_type=F32))
    hidden = (hidden * jnp.dot(rows, w_up, preferred_element_type=F32)).astype(BF16)
    return jnp.dot(hidden, w_down, preferred_element_type=F32)


def exchange(rows):
    return lax.all_to_all(rows, SP_TP, split_axis=0, concat_axis=0, tiled=True)


def routes(index, weight, experts, room):
    length = index.shape[0]
    ids = jnp.arange(experts, dtype=jnp.int32)[:, None]
    named = jnp.zeros((experts, length), F32)
    weights = jnp.zeros((experts, length), F32)
    for j in range(index.shape[1]):
        here = index[:, j][None, :] == ids
        named = named + here.astype(F32)
        weights = weights + jnp.where(here, weight[:, j][None, :], 0.0)
    place = jnp.arange(length, dtype=jnp.int32)
    earlier = (place[:, None] < place[None, :]).astype(BF16)
    slot = jnp.dot(named.astype(BF16), earlier, preferred_element_type=F32)
    slot = jnp.where(named > 0, slot, -1.0)[:, None, :]
    step = jnp.arange(KEEP, dtype=jnp.int32)[None, :, None]
    extra = room - KEEP
    first = slot == step.astype(F32)
    rest = slot == (KEEP + step % extra).astype(F32)
    lead = rest & (step < extra)
    tail = rest & (step >= extra)
    weights = weights[:, None, :]

    def flat(mask):
        return mask.reshape(experts * KEEP, length)

    out = [flat(m.astype(BF16)) for m in (first, lead, tail)]
    back = [flat(jnp.where(m, weights, 0.0).astype(BF16)) for m in (first, lead, tail)]
    return out, back


def shards(
    projected_queries,
    projected_keys,
    projected_values,
    output_gate_values,
    write_strength_logits,
    decay_input_logits,
    head_rate_logarithm,
    extra_log_decay,
    per_head_norm_gain,
    output_matrix,
    residual,
    mixture_norm_gain,
    selected_expert_index,
    routing_weight,
    routed_gate_weight,
    routed_up_weight,
    routed_down_weight,
    common_gate_weight,
    common_up_weight,
    common_down_weight,
):
    place = place_on("sp_2")
    maps, qe, o0 = block_terms(
        projected_queries,
        projected_keys,
        projected_values,
        write_strength_logits,
        decay_input_logits,
        head_rate_logarithm,
        extra_log_decay,
        place,
    )
    states = entering(maps, place)
    keep, send = finish(qe, o0, states, output_gate_values, per_head_norm_gain, place)
    came = ring(send, "tp", 1)
    wide = keep.shape[1]
    length = residual.shape[0]
    first_core = lax.axis_index("tp") == 0
    projected = jnp.dot(
        jnp.where(first_core, keep, came), output_matrix[:wide], preferred_element_type=F32
    ) + jnp.dot(
        jnp.where(first_core, came, keep), output_matrix[wide:], preferred_element_type=F32
    )
    attended = (residual.astype(F32) + projected).astype(BF16)
    normed = normalize(attended.astype(F32), mixture_norm_gain)

    experts = lax.axis_size(SP) * lax.axis_size("tp")
    room = max(2, length * TOP_K * 3 // (2 * experts))
    extra = room - KEEP
    dim = normed.shape[1]
    half = dim // 2
    (first, lead, tail), (w_first, w_lead, w_tail) = routes(
        selected_expert_index, routing_weight, experts, room
    )
    main_out = jnp.dot(first, normed, preferred_element_type=F32).astype(BF16)
    rest_out = (
        jnp.dot(lead, normed[:, :half], preferred_element_type=F32)
        + jnp.dot(tail, normed[:, half:], preferred_element_type=F32)
    ).astype(BF16)
    main_in = exchange(main_out.reshape(experts, KEEP, dim))
    rest_in = exchange(rest_out.reshape(experts, KEEP, half))
    shared = feed_forward(normed, common_gate_weight, common_up_weight, common_down_weight)

    weights = (routed_gate_weight[0], routed_up_weight[0], routed_down_weight[0])
    main_rows = feed_forward(main_in.reshape(experts * KEEP, dim), *weights).astype(BF16)
    main_back = exchange(main_rows.reshape(experts, KEEP, dim)).reshape(experts * KEEP, dim)
    unfolded = rest_in.reshape(experts, 2, extra, half).transpose(0, 2, 1, 3)
    rest_rows = feed_forward(unfolded.reshape(experts * extra, dim), *weights).astype(BF16)
    folded = rest_rows.reshape(experts, extra, 2, half).transpose(0, 2, 1, 3)
    rest_back = exchange(folded.reshape(experts, KEEP, half)).reshape(experts * KEEP, half)

    def combine(table, rows):
        return lax.dot_general(table, rows, (((0,), (0,)), ((), ())), preferred_element_type=F32)

    early = jnp.concatenate([combine(w_lead, rest_back), combine(w_tail, rest_back)], axis=1)
    early = early + attended.astype(F32) + shared
    early, table = lax.optimization_barrier((early, w_first.T))
    return (early + jnp.dot(table, main_back, preferred_element_type=F32)).astype(BF16)


def solution(mesh):
    finer = Mesh(mesh.devices.reshape(4, 4, 4, mesh.shape["tp"]), ("sp_0", "sp_1", "sp_2", "tp"))
    in_specs = (
        P(SP, "tp"),
        P(SP, "tp"),
        P(SP, "tp"),
        P(SP, "tp"),
        P(SP, "tp"),
        P(SP, "tp"),
        P("tp"),
        P(SP, "tp"),
        P(),
        P(),
        P(SP_TP, None),
        P(),
        P(SP_TP, None),
        P(SP_TP, None),
        P(SP_TP, None, None),
        P(SP_TP, None, None),
        P(SP_TP, None, None),
        P(),
        P(),
        P(),
    )
    out_specs = P(SP_TP, None)
    return jax.shard_map(
        shards, mesh=finer, in_specs=in_specs, out_specs=out_specs, check_vma=False
    )
```

```python
import functools

import jax
import jax.numpy as jnp
from jax import lax
from jax.experimental import pallas as pl
from jax.experimental.pallas import tpu as pltpu
from jax.sharding import Mesh
from jax.sharding import PartitionSpec as P

TOP_K = 4
HD = 128
BLOCK = 128
KEEP = 8
SP = ("sp_0", "sp_1", "sp_2")
SP_TP = ("sp_0", "sp_1", "sp_2", "tp")
EPS = 1e-06
F32 = jnp.float32
BF16 = jnp.bfloat16


def dot_nn(a, b):
    return lax.dot_general(a, b, (((1,), (0,)), ((), ())), preferred_element_type=F32)


def dot_nt(a, b):
    return lax.dot_general(a, b, (((1,), (1,)), ((), ())), preferred_element_type=F32)


def dot_tn(a, b):
    return lax.dot_general(a, b, (((0,), (0,)), ((), ())), preferred_element_type=F32)


def parts(x):
    high = x.astype(BF16)
    return high, (x - high.astype(F32)).astype(BF16)


def rows_of(*arrays):
    return jnp.concatenate(arrays, axis=0)


def cols_of(*arrays):
    return jnp.concatenate(arrays, axis=1)


def fine(a, b):
    ah, al = a
    bh, bl = b
    return dot_nn(cols_of(ah, al), rows_of(bh, bh)) + dot_nn(ah, bl)


def fine_square(a, b):
    ah, al = a
    bh, bl = b
    both = dot_nn(cols_of(ah, al), rows_of(cols_of(bh, bl), cols_of(bh, jnp.zeros_like(bl))))
    return both[:, :HD] + both[:, HD:]


def own_row(ref, head):
    table = ref[...].astype(F32)
    which = lax.broadcasted_iota(jnp.int32, table.shape, 0)
    return jnp.sum(jnp.where(which == head, table, 0.0), axis=0, keepdims=True)


def decay_sums(rate_ref, decay_ref, extra_ref, head):
    length = decay_ref.shape[1]
    raw = own_row(decay_ref, head) - 6.0
    soft = jnp.maximum(raw, 0.0) + jnp.log1p(jnp.exp(-jnp.abs(raw)))
    rate = jnp.exp(jnp.full((1, length), rate_ref[head], F32))
    total = jnp.broadcast_to(own_row(extra_ref, head) - rate * soft, (8, length))
    lane = lax.broadcasted_iota(jnp.int32, total.shape, 1)
    shift = 1
    while shift < length:
        total = total + jnp.where(lane >= shift, pltpu.roll(total, shift, 1), 0.0)
        shift *= 2
    g_row = total[0:1, :]
    return g_row, jnp.broadcast_to(g_row, (HD, length)).T


def unit(ref):
    x = ref[...].astype(F32)
    active = x * jax.nn.sigmoid(x)
    return active * lax.rsqrt(jnp.sum(active * active, axis=-1, keepdims=True) + EPS)


def against_keys(left, keys, number, g_row, g_col):
    ii = lax.broadcasted_iota(jnp.int32, (BLOCK, BLOCK), 0)
    jj = lax.broadcasted_iota(jnp.int32, (BLOCK, BLOCK), 1)
    blocks = []
    for r in range(number):
        here = slice(r * BLOCK, (r + 1) * BLOCK)
        upto = slice(0, (r + 1) * BLOCK)
        high = keys[0][upto]
        both = dot_nt(cols_of(left[0][here], left[1][here]), cols_of(high, high))
        both = both + dot_nt(left[0][here], keys[1][upto])
        row = []
        for c in range(r + 1):
            there = slice(c * BLOCK, (c + 1) * BLOCK)
            gap = g_col[here] - g_row[:, there]
            if c == r:
                gap = jnp.where(ii >= jj, gap, -1e30)
            row.append(both[:, there] * jnp.exp(gap))
        blocks.append(row)
    return blocks


def head_at(slots, step, place, heads):
    return (place + jnp.where(step == 0, slots[0], slots[1])) % heads


def maps_kernel(slots, place_ref, rate_ref, k_ref, v_ref, write_ref, decay_ref, extra_ref, *refs):
    one_ref, two_ref, high_ref, low_ref = refs[-4:]
    length = k_ref.shape[0]
    number = length // BLOCK
    step = pl.program_id(0)
    head = head_at(slots, step, place_ref[0], rate_ref.shape[0])
    g_row, g_col = decay_sums(rate_ref, decay_ref, extra_ref, head)
    beta = jax.nn.sigmoid(own_row(write_ref, head))
    b_col = jnp.broadcast_to(beta, (HD, length)).T
    keys = unit(k_ref)
    raw = v_ref[...].astype(F32)
    values = raw * jax.nn.sigmoid(raw)
    k_beta = keys * b_col
    right = cols_of(k_beta * jnp.exp(g_col), values * b_col)
    g_last = g_col[length - 1 : length, :]
    k_late = parts(keys * jnp.exp(g_last - g_col))
    lower = against_keys(parts(k_beta), parts(keys), number, g_row, g_col)
    ii = lax.broadcasted_iota(jnp.int32, (BLOCK, BLOCK), 0)
    jj = lax.broadcasted_iota(jnp.int32, (BLOCK, BLOCK), 1)
    eye = (ii == jj).astype(F32)
    near = (ii // 2 == jj // 2) & (ii > jj)
    inverse = [eye - jnp.where(near, lower[r][r], 0.0) for r in range(number)]

    def widen(level, inverse):
        chosen = (ii >> (level + 1) == jj >> (level + 1)) & (ii >> level > jj >> level)
        halves = [parts(t) for t in inverse]
        steps = [
            fine_square(halves[r], parts(jnp.where(chosen, lower[r][r], 0.0)))
            for r in range(number)
        ]
        return [inverse[r] - fine_square(parts(steps[r]), halves[r]) for r in range(number)]

    inverse = lax.fori_loop(1, BLOCK.bit_length() - 1, widen, inverse)
    highs, lows = [], []
    for r in range(number):
        here = slice(r * BLOCK, (r + 1) * BLOCK)
        rest = right[here]
        if r > 0:
            known = (rows_of(*highs), rows_of(*lows))
            rest = rest - fine(parts(cols_of(*lower[r][:r])), known)
        one = parts(fine(parts(inverse[r]), parts(rest)))
        highs.append(one[0])
        lows.append(one[1])
        high_ref[here, :] = one[0]
        low_ref[here, :] = one[1]
    high, low = rows_of(*highs), rows_of(*lows)
    moved = dot_tn(rows_of(*k_late), rows_of(high, high)) + dot_tn(k_late[0], low)
    whole = cols_of(eye * jnp.exp(g_last) - moved[:, :HD], moved[:, HD:])
    for k, map_ref in enumerate((one_ref, two_ref)):

        @pl.when(step == k)
        def _(map_ref=map_ref):
            map_ref[...] = whole


def mixes_kernel(rate_ref, q_ref, k_ref, decay_ref, extra_ref, high_ref, low_ref, qe_ref, o0_ref):
    length = q_ref.shape[0]
    number = length // BLOCK
    g_row, g_col = decay_sums(rate_ref, decay_ref, extra_ref, pl.program_id(0))
    queries = unit(q_ref)
    mixing = against_keys(parts(queries), parts(unit(k_ref)), number, g_row, g_col)
    grown = queries * jnp.exp(g_col)
    for r in range(number):
        here = slice(r * BLOCK, (r + 1) * BLOCK)
        upto = slice(0, (r + 1) * BLOCK)
        mixed = fine(parts(cols_of(*mixing[r])), (high_ref[upto, :], low_ref[upto, :]))
        qe_ref[here, :] = grown[here] - mixed[:, :HD]
        o0_ref[here, :] = mixed[:, HD:]


def state_maps(slots, keys, values, write_logits, decays, rates, place, filled):
    length, wide = keys.shape
    heads = wide // HD

    def whose(step, place_ref):
        return 0, head_at(slots, step, place_ref[0], heads)

    column = pl.BlockSpec((length, HD), whose)
    double = pl.BlockSpec((length, 2 * HD), whose)
    table = pl.BlockSpec((heads, length), lambda step, place_ref: (0, 0))
    small = pl.BlockSpec(memory_space=pltpu.SMEM)
    one_map = pl.BlockSpec((HD, 2 * HD), lambda step, place_ref: (0, 0))
    kept = [pl.BlockSpec(memory_space=pl.ANY)] * len(filled)
    return pl.pallas_call(
        functools.partial(maps_kernel, slots),
        grid_spec=pltpu.PrefetchScalarGridSpec(
            num_scalar_prefetch=1,
            grid=(2,),
            in_specs=[small, column, column, table, table, table] + kept,
            out_specs=[one_map, one_map, double, double],
        ),
        out_shape=[pltpu.VMEM((HD, 2 * HD), F32)] * 2
        + [jax.ShapeDtypeStruct((length, 2 * wide), BF16)] * 2,
        input_output_aliases={7: 2, 8: 3} if filled else {},
        name="maps",
    )(place, rates, keys, values, write_logits.T, *decays, *filled)


def mixes(queries, keys, decays, rates, high, low):
    length, wide = queries.shape
    heads = wide // HD
    column = pl.BlockSpec((length, HD), lambda h: (0, h))
    double = pl.BlockSpec((length, 2 * HD), lambda h: (0, h))
    table = pl.BlockSpec((heads, length), lambda h: (0, 0))
    small = pl.BlockSpec(memory_space=pltpu.SMEM)
    return pl.pallas_call(
        mixes_kernel,
        grid=(heads,),
        in_specs=[small, column, column, table, table, double, double],
        out_specs=[column, column],
        out_shape=[jax.ShapeDtypeStruct((length, wide), F32)] * 2,
        name="mixes",
    )(rates, queries, keys, *decays, high, low)


def shift_in(later):
    wide = lax.broadcasted_iota(jnp.int32, later.shape, 1)
    return jnp.where(wide >= HD, later, 0.0)


def then(later, earlier):
    return fine(parts(later[:, :HD]), parts(earlier)) + shift_in(later)


def identity_map():
    ii = lax.broadcasted_iota(jnp.int32, (HD, 2 * HD), 0)
    jj = lax.broadcasted_iota(jnp.int32, (HD, 2 * HD), 1)
    return (ii == jj).astype(F32)


def in_order(place, refs, held_ref):
    number = len(refs)
    for s, ref in enumerate(refs):
        held_ref[(place + number - s) % number] = ref[...]


def all_before_kernel(place_ref, *refs):
    maps, (before_ref, total_ref, held_ref) = refs[:-3], refs[-3:]
    in_order(place_ref[0], maps, held_ref)
    running = identity_map()
    for k in range(len(maps)):
        before_ref[k] = running
        running = held_ref[k] if k == 0 else then(held_ref[k], running)
    total_ref[...] = running


def mine_before_kernel(place_ref, *refs):
    maps, (before_ref, total_ref, held_ref) = refs[:-3], refs[-3:]
    place = place_ref[0]
    in_order(place, maps, held_ref)
    running = identity_map()
    before_ref[...] = running
    for k in range(len(maps)):
        running = held_ref[k] if k == 0 else then(held_ref[k], running)

        @pl.when(place == k + 1)
        def _(running=running):
            before_ref[...] = running

    total_ref[...] = running


def small_call(kernel, out_shape, scratch, place, *arrays):
    return pl.pallas_call(
        kernel,
        in_specs=[pl.BlockSpec(memory_space=pltpu.SMEM)]
        + [pl.BlockSpec(memory_space=pltpu.VMEM)] * len(arrays),
        out_shape=out_shape,
        scratch_shapes=scratch,
        compiler_params=pltpu.CompilerParams(vmem_limit_bytes=8 << 20),
    )(place, *[pltpu.with_memory_space_constraint(a, pltpu.VMEM) for a in arrays])


def states_kernel(place_ref, one_ref, two_ref, three_ref, middle_ref, inner_ref, *out_refs):
    state = three_ref[:, HD:]
    for ref in (two_ref, one_ref, middle_ref):
        state = fine(parts(ref[:, :HD]), parts(state)) + ref[:, HD:]
    pair = parts(state)
    number = len(out_refs)
    for s, out_ref in enumerate(out_refs):
        k = (place_ref[0] + number - s) % number
        out_ref[...] = fine(parts(inner_ref[k, :, :HD]), pair) + inner_ref[k, :, HD:]


def ring(array, axis, step):
    count = lax.axis_size(axis)
    return lax.ppermute(array, axis, [(i, (i + step) % count) for i in range(count)])


def onward(array, axis, step):
    count = lax.axis_size(axis)
    return lax.ppermute(array, axis, [(i, i + step) for i in range(count - step)])


def place_on(axis):
    return lax.axis_index(axis).reshape(1).astype(jnp.int32)


def entering(own, arrived, place):
    number = 1 + len(arrived)
    one = pltpu.VMEM(own.shape, F32)
    many = pltpu.VMEM((number,) + own.shape, F32)
    held = [pltpu.VMEM((number,) + own.shape, F32)]
    inner, line = small_call(all_before_kernel, [many, one], held, place, own, *arrived)
    two = ring(line, "sp_1", 2)
    first, three = [ring(line, "sp_1", s) for s in (1, 3)]
    middle, plane = small_call(
        mine_before_kernel, [one, one], held, place_on("sp_1"), line, first, two, three
    )
    two, first, three = [onward(plane, "sp_0", s) for s in (2, 1, 3)]
    found = small_call(
        states_kernel,
        [pltpu.VMEM((HD, HD), F32)] * number,
        (),
        place,
        first,
        two,
        three,
        middle,
        inner,
    )
    two, first, three = [ring(found[s], "sp_2", number - s) for s in (2, 1, 3)]
    return [found[0], first, two, three]


def finish_kernel(place_ref, core_ref, qe_ref, o0_ref, gate_ref, gain_ref, *refs):
    states, (keep_ref, send_ref, whole_ref) = refs[:-3], refs[-3:]
    number = len(states)
    half = keep_ref.shape[0]
    core = core_ref[0]

    @pl.loop(0, number)
    def _(h):
        there = pl.ds(pl.multiple_of(h * HD, HD), HD)
        slot = (h + number - place_ref[0]) % number
        state = states[0][...]
        for s in range(1, number):
            state = jnp.where(slot == s, states[s][...], state)
        mix = o0_ref[:, there] + fine(parts(qe_ref[:, there]), parts(state))
        scaled = mix * lax.rsqrt(jnp.mean(mix * mix, axis=-1, keepdims=True) + EPS)
        gate = gate_ref[:, there].astype(F32)
        whole_ref[...] = scaled * gain_ref[...] * (gate * jax.nn.sigmoid(gate))
        keep_ref[:, there] = whole_ref[pl.ds(core * half, half), :].astype(BF16)
        send_ref[:, there] = whole_ref[pl.ds((1 - core) * half, half), :].astype(BF16)


def finish(qe, o0, states, gate, gain, place):
    length, wide = qe.shape
    small = pl.BlockSpec(memory_space=pltpu.SMEM)
    arrays = (qe, o0, gate, gain.reshape(1, HD), *states)
    return pl.pallas_call(
        finish_kernel,
        in_specs=[small, small] + [pl.BlockSpec(memory_space=pltpu.VMEM)] * len(arrays),
        out_shape=[pltpu.VMEM((length // 2, wide), BF16)] * 2,
        scratch_shapes=[pltpu.VMEM((length, HD), F32)],
        compiler_params=pltpu.CompilerParams(vmem_limit_bytes=12 << 20),
        name="finish",
    )(
        place,
        place_on("tp"),
        *[pltpu.with_memory_space_constraint(a, pltpu.VMEM) for a in arrays],
    )


def feed_forward(rows, w_gate, w_up, w_down):
    hidden = jax.nn.silu(jnp.dot(rows, w_gate, preferred_element_type=F32))
    hidden = (hidden * jnp.dot(rows, w_up, preferred_element_type=F32)).astype(BF16)
    return jnp.dot(hidden, w_down, preferred_element_type=F32)


def exchange(rows):
    return lax.all_to_all(rows, SP_TP, split_axis=0, concat_axis=0, tiled=True)


def routes(index, weight, experts, room):
    length = index.shape[0]
    ids = jnp.arange(experts, dtype=jnp.int32)[:, None]
    named = jnp.zeros((experts, length), F32)
    weights = jnp.zeros((experts, length), F32)
    for j in range(index.shape[1]):
        here = index[:, j][None, :] == ids
        named = named + here.astype(F32)
        weights = weights + jnp.where(here, weight[:, j][None, :], 0.0)
    place = jnp.arange(length, dtype=jnp.int32)
    earlier = (place[:, None] < place[None, :]).astype(BF16)
    slot = jnp.dot(named.astype(BF16), earlier, preferred_element_type=F32)
    plain = jnp.where(named > 0, slot, -1.0)
    slot = plain[:, None, :]
    step = jnp.arange(KEEP, dtype=jnp.int32)[None, :, None]
    extra = room - KEEP
    first = slot == step.astype(F32)
    rest = slot == (KEEP + step % extra).astype(F32)
    lead = rest & (step < extra)
    tail = rest & (step >= extra)
    weights = weights[:, None, :]

    def flat(mask):
        return mask.reshape(experts * KEEP, length)

    back = [flat(jnp.where(m, weights, 0.0).astype(BF16)) for m in (first, lead, tail)]
    return plain, back


def places(slot_ref, start, count, length):
    slot = slot_ref[pl.ds(start, count), :]
    slot = jnp.broadcast_to(slot[:, None, :], (count, KEEP, length)).reshape(count * KEEP, length)
    step = lax.broadcasted_iota(jnp.int32, (count * KEEP, length), 0) % KEEP
    return slot, step


def attend_kernel(
    core_ref, keep_ref, came_ref, gain_ref, slot_ref, matrix_ref, residual_ref, *refs
):
    attended_ref, normed_ref, rest_ref, wide_ref, matrix_vmem, residual_vmem, done = refs
    length, dim = residual_ref.shape
    wide = keep_ref.shape[1]
    number = 4
    block = dim // number
    copies = [pltpu.make_async_copy(residual_ref, residual_vmem, done.at[number])]
    for c in range(number):
        there = pl.ds(c * block, block)
        copies.append(
            pltpu.make_async_copy(matrix_ref.at[:, there], matrix_vmem.at[:, there], done.at[c])
        )
    for copy in copies:
        copy.start()
    keep, came = keep_ref[...].astype(F32), came_ref[...].astype(F32)
    first_core = core_ref[0] == 0
    lead = jnp.where(first_core, keep, came).astype(BF16)
    tail = jnp.where(first_core, came, keep).astype(BF16)
    copies[0].wait()
    squares = jnp.zeros((length, 1), F32)
    for c in range(number):
        there = slice(c * block, (c + 1) * block)
        copies[1 + c].wait()
        projected = dot_nn(lead, matrix_vmem[:wide, there]) + dot_nn(tail, matrix_vmem[wide:, there])
        attended = (residual_vmem[:, there].astype(F32) + projected).astype(BF16)
        attended_ref[:, there] = attended
        plain = attended.astype(F32)
        wide_ref[:, there] = plain
        squares = squares + jnp.sum(plain * plain, axis=-1, keepdims=True)
    scale = lax.rsqrt(squares / dim + EPS)
    normed_ref[...] = (wide_ref[...] * scale * gain_ref[...]).astype(BF16)
    half = dim // 2
    count = 32

    @pl.loop(0, slot_ref.shape[0] // count)
    def _(i):
        start = pl.multiple_of(i * count, count)
        slot, step = places(slot_ref, start, count, length)
        extra = KEEP // 2
        chosen = slot == (KEEP + step % extra).astype(F32)
        lead = (chosen & (step < extra)).astype(F32).astype(BF16)
        tail = (chosen & (step >= extra)).astype(F32).astype(BF16)
        rows = dot_nn(lead, normed_ref[:, :half]) + dot_nn(tail, normed_ref[:, half:])
        rest_ref[pl.ds(start, count), :, :] = rows.astype(BF16).reshape(count, KEEP, half)


def attend(keep, came, out_matrix, residual, gain, slot):
    length, dim = residual.shape
    experts = slot.shape[0]
    arrays = (keep, came, gain.reshape(1, dim), slot)
    rows = pltpu.HBM((length, dim), BF16)
    return pl.pallas_call(
        attend_kernel,
        in_specs=[pl.BlockSpec(memory_space=pltpu.SMEM)]
        + [pl.BlockSpec(memory_space=pltpu.VMEM)] * len(arrays)
        + [pl.BlockSpec(memory_space=pl.ANY)] * 2,
        out_shape=[rows, rows, pltpu.HBM((experts, KEEP, dim // 2), BF16)],
        scratch_shapes=[
            pltpu.VMEM((length, dim), F32),
            pltpu.VMEM(out_matrix.shape, BF16),
            pltpu.VMEM((length, dim), BF16),
            pltpu.SemaphoreType.DMA((5,)),
        ],
        name="attend",
    )(
        place_on("tp"),
        *[pltpu.with_memory_space_constraint(a, pltpu.VMEM) for a in arrays],
        out_matrix,
        residual,
    )


def dispatch_kernel(slot_ref, normed_ref, out_ref):
    count, _, dim = out_ref.shape
    start = pl.multiple_of(pl.program_id(0) * count, count)
    slot, step = places(slot_ref, start, count, normed_ref.shape[0])
    chosen = (slot == step.astype(F32)).astype(F32).astype(BF16)
    rows = dot_nn(chosen, normed_ref[...]).astype(BF16)
    out_ref[...] = rows.reshape(count, KEEP, dim)


def dispatch(slot, normed):
    experts, length = slot.shape
    dim = normed.shape[1]
    count = 16
    return pl.pallas_call(
        dispatch_kernel,
        grid=(experts // count,),
        in_specs=[
            pl.BlockSpec((experts, length), lambda i: (0, 0)),
            pl.BlockSpec((length, dim), lambda i: (0, 0)),
        ],
        out_specs=pl.BlockSpec((count, KEEP, dim), lambda i: (i, 0, 0)),
        out_shape=jax.ShapeDtypeStruct((experts, KEEP, dim), BF16),
        name="dispatch",
    )(slot, normed)


def final_kernel(table_ref, rows_ref, early_ref, out_ref):
    out_ref[...] = (early_ref[...] + dot_nn(table_ref[...], rows_ref[...])).astype(BF16)


def final_sum(table, rows, early):
    length, wide = early.shape
    block = wide // 8
    column = pl.BlockSpec((length, block), lambda i: (0, i))
    return pl.pallas_call(
        final_kernel,
        grid=(wide // block,),
        in_specs=[
            pl.BlockSpec(table.shape, lambda i: (0, 0)),
            pl.BlockSpec((rows.shape[0], block), lambda i: (0, i)),
            column,
        ],
        out_specs=column,
        out_shape=jax.ShapeDtypeStruct((length, wide), BF16),
        name="final_sum",
    )(table, rows, early)


def shards(
    projected_queries,
    projected_keys,
    projected_values,
    output_gate_values,
    write_strength_logits,
    decay_input_logits,
    head_rate_logarithm,
    extra_log_decay,
    per_head_norm_gain,
    output_matrix,
    residual,
    mixture_norm_gain,
    selected_expert_index,
    routing_weight,
    routed_gate_weight,
    routed_up_weight,
    routed_down_weight,
    common_gate_weight,
    common_up_weight,
    common_down_weight,
):
    place = place_on("sp_2")
    decays = (decay_input_logits.T, extra_log_decay.T)
    base = (projected_keys, projected_values, write_strength_logits, decays, head_rate_logarithm)
    far, near, high, low = state_maps((2, 1), *base, place, ())
    far = ring(far, "sp_2", 2)
    near = ring(near, "sp_2", 1)
    last, own, high, low = state_maps((3, 0), *base, place, (high, low))
    states = entering(own, (near, far, ring(last, "sp_2", 3)), place)
    qe, o0 = mixes(projected_queries, projected_keys, decays, head_rate_logarithm, high, low)
    keep, send = finish(qe, o0, states, output_gate_values, per_head_norm_gain, place)
    came = ring(send, "tp", 1)
    length, dim = residual.shape
    experts = lax.axis_size(SP) * lax.axis_size("tp")
    room = max(2, length * TOP_K * 3 // (2 * experts))
    extra = room - KEEP
    half = dim // 2
    slot, (w_first, w_lead, w_tail) = routes(selected_expert_index, routing_weight, experts, room)
    attended, normed, rest_out = attend(
        keep, came, output_matrix, residual, mixture_norm_gain, slot
    )
    rest_in = exchange(rest_out)
    main_in = exchange(dispatch(slot, normed))
    shared = feed_forward(normed, common_gate_weight, common_up_weight, common_down_weight)

    weights = (routed_gate_weight[0], routed_up_weight[0], routed_down_weight[0])
    main_rows = feed_forward(main_in.reshape(experts * KEEP, dim), *weights).astype(BF16)
    main_back = exchange(main_rows.reshape(experts, KEEP, dim)).reshape(experts * KEEP, dim)
    unfolded = rest_in.reshape(experts, 2, extra, half).transpose(0, 2, 1, 3)
    rest_rows = feed_forward(unfolded.reshape(experts * extra, dim), *weights).astype(BF16)
    folded = rest_rows.reshape(experts, extra, 2, half).transpose(0, 2, 1, 3)
    rest_back = exchange(folded.reshape(experts, KEEP, half)).reshape(experts * KEEP, half)

    def combine(table, rows):
        return lax.dot_general(table, rows, (((0,), (0,)), ((), ())), preferred_element_type=F32)

    early = jnp.concatenate([combine(w_lead, rest_back), combine(w_tail, rest_back)], axis=1)
    early = early + attended.astype(F32) + shared
    return final_sum(w_first.T, main_back, early)


def solution(mesh):
    finer = Mesh(mesh.devices.reshape(4, 4, 4, mesh.shape["tp"]), ("sp_0", "sp_1", "sp_2", "tp"))
    in_specs = (
        P(SP, "tp"),
        P(SP, "tp"),
        P(SP, "tp"),
        P(SP, "tp"),
        P(SP, "tp"),
        P(SP, "tp"),
        P("tp"),
        P(SP, "tp"),
        P(),
        P(),
        P(SP_TP, None),
        P(),
        P(SP_TP, None),
        P(SP_TP, None),
        P(SP_TP, None, None),
        P(SP_TP, None, None),
        P(SP_TP, None, None),
        P(),
        P(),
        P(),
    )
    out_specs = P(SP_TP, None)

    return jax.shard_map(
        shards, mesh=finer, in_specs=in_specs, out_specs=out_specs, check_vma=False
    )
```

```python
import functools

import jax
import jax.numpy as jnp
from jax import lax
from jax.experimental import pallas as pl
from jax.experimental.pallas import tpu as pltpu
from jax.sharding import Mesh
from jax.sharding import PartitionSpec as P

TOP_K = 4
HD = 128
BLOCK = 128
KEEP = 8
SP = ("sp_0", "sp_1", "sp_2")
SP_TP = ("sp_0", "sp_1", "sp_2", "tp")
EPS = 1e-06
F32 = jnp.float32
BF16 = jnp.bfloat16


def dot_nn(a, b):
    return lax.dot_general(a, b, (((1,), (0,)), ((), ())), preferred_element_type=F32)


def dot_nt(a, b):
    return lax.dot_general(a, b, (((1,), (1,)), ((), ())), preferred_element_type=F32)


def dot_tn(a, b):
    return lax.dot_general(a, b, (((0,), (0,)), ((), ())), preferred_element_type=F32)


def parts(x):
    high = x.astype(BF16)
    return high, (x - high.astype(F32)).astype(BF16)


def rows_of(*arrays):
    return jnp.concatenate(arrays, axis=0)


def cols_of(*arrays):
    return jnp.concatenate(arrays, axis=1)


def fine(a, b):
    ah, al = a
    bh, bl = b
    return dot_nn(cols_of(ah, al), rows_of(bh, bh)) + dot_nn(ah, bl)


def fine_square(a, b):
    ah, al = a
    bh, bl = b
    both = dot_nn(cols_of(ah, al), rows_of(cols_of(bh, bl), cols_of(bh, jnp.zeros_like(bl))))
    return both[:, :HD] + both[:, HD:]


def own_row(ref, head):
    table = ref[...].astype(F32)
    which = lax.broadcasted_iota(jnp.int32, table.shape, 0)
    return jnp.sum(jnp.where(which == head, table, 0.0), axis=0, keepdims=True)


def decay_sums(rate_ref, decay_ref, extra_ref, head):
    length = decay_ref.shape[1]
    raw = own_row(decay_ref, head) - 6.0
    soft = jnp.maximum(raw, 0.0) + jnp.log1p(jnp.exp(-jnp.abs(raw)))
    rate = jnp.exp(jnp.full((1, length), rate_ref[head], F32))
    total = jnp.broadcast_to(own_row(extra_ref, head) - rate * soft, (8, length))
    lane = lax.broadcasted_iota(jnp.int32, total.shape, 1)
    shift = 1
    while shift < length:
        total = total + jnp.where(lane >= shift, pltpu.roll(total, shift, 1), 0.0)
        shift *= 2
    g_row = total[0:1, :]
    return g_row, jnp.broadcast_to(g_row, (HD, length)).T


def unit(ref):
    x = ref[...].astype(F32)
    active = x * jax.nn.sigmoid(x)
    return active * lax.rsqrt(jnp.sum(active * active, axis=-1, keepdims=True) + EPS)


def against_keys(left, keys, number, g_row, g_col):
    ii = lax.broadcasted_iota(jnp.int32, (BLOCK, BLOCK), 0)
    jj = lax.broadcasted_iota(jnp.int32, (BLOCK, BLOCK), 1)
    blocks = []
    for r in range(number):
        here = slice(r * BLOCK, (r + 1) * BLOCK)
        upto = slice(0, (r + 1) * BLOCK)
        high = keys[0][upto]
        both = dot_nt(cols_of(left[0][here], left[1][here]), cols_of(high, high))
        both = both + dot_nt(left[0][here], keys[1][upto])
        row = []
        for c in range(r + 1):
            there = slice(c * BLOCK, (c + 1) * BLOCK)
            gap = g_col[here] - g_row[:, there]
            if c == r:
                gap = jnp.where(ii >= jj, gap, -1e30)
            row.append(both[:, there] * jnp.exp(gap))
        blocks.append(row)
    return blocks


def head_at(slots, step, place, heads):
    return (place + jnp.where(step == 0, slots[0], slots[1])) % heads


def maps_kernel(slots, place_ref, rate_ref, k_ref, v_ref, write_ref, decay_ref, extra_ref, *refs):
    one_ref, two_ref, high_ref, low_ref = refs[-4:]
    length = k_ref.shape[0]
    number = length // BLOCK
    step = pl.program_id(0)
    head = head_at(slots, step, place_ref[0], rate_ref.shape[0])
    g_row, g_col = decay_sums(rate_ref, decay_ref, extra_ref, head)
    beta = jax.nn.sigmoid(own_row(write_ref, head))
    b_col = jnp.broadcast_to(beta, (HD, length)).T
    keys = unit(k_ref)
    raw = v_ref[...].astype(F32)
    values = raw * jax.nn.sigmoid(raw)
    k_beta = keys * b_col
    right = cols_of(k_beta * jnp.exp(g_col), values * b_col)
    g_last = g_col[length - 1 : length, :]
    k_late = parts(keys * jnp.exp(g_last - g_col))
    lower = against_keys(parts(k_beta), parts(keys), number, g_row, g_col)
    ii = lax.broadcasted_iota(jnp.int32, (BLOCK, BLOCK), 0)
    jj = lax.broadcasted_iota(jnp.int32, (BLOCK, BLOCK), 1)
    eye = (ii == jj).astype(F32)
    near = (ii // 2 == jj // 2) & (ii > jj)
    inverse = [eye - jnp.where(near, lower[r][r], 0.0) for r in range(number)]

    def widen(level, inverse):
        chosen = (ii >> (level + 1) == jj >> (level + 1)) & (ii >> level > jj >> level)
        halves = [parts(t) for t in inverse]
        steps = [
            fine_square(halves[r], parts(jnp.where(chosen, lower[r][r], 0.0)))
            for r in range(number)
        ]
        return [inverse[r] - fine_square(parts(steps[r]), halves[r]) for r in range(number)]

    for level in range(1, BLOCK.bit_length() - 1):
        inverse = widen(level, inverse)
    highs, lows = [], []
    for r in range(number):
        here = slice(r * BLOCK, (r + 1) * BLOCK)
        rest = right[here]
        if r > 0:
            known = (rows_of(*highs), rows_of(*lows))
            rest = rest - fine(parts(cols_of(*lower[r][:r])), known)
        one = parts(fine(parts(inverse[r]), parts(rest)))
        highs.append(one[0])
        lows.append(one[1])
        high_ref[here, :] = one[0]
        low_ref[here, :] = one[1]
    high, low = rows_of(*highs), rows_of(*lows)
    moved = dot_tn(rows_of(*k_late), rows_of(high, high)) + dot_tn(k_late[0], low)
    whole = cols_of(eye * jnp.exp(g_last) - moved[:, :HD], moved[:, HD:])
    for k, map_ref in enumerate((one_ref, two_ref)):

        @pl.when(step == k)
        def _(map_ref=map_ref):
            map_ref[...] = whole


def mixes_kernel(rate_ref, q_ref, k_ref, decay_ref, extra_ref, high_ref, low_ref, qe_ref, o0_ref):
    length = q_ref.shape[0]
    number = length // BLOCK
    g_row, g_col = decay_sums(rate_ref, decay_ref, extra_ref, pl.program_id(0))
    queries = unit(q_ref)
    mixing = against_keys(parts(queries), parts(unit(k_ref)), number, g_row, g_col)
    grown = queries * jnp.exp(g_col)
    for r in range(number):
        here = slice(r * BLOCK, (r + 1) * BLOCK)
        upto = slice(0, (r + 1) * BLOCK)
        mixed = fine(parts(cols_of(*mixing[r])), (high_ref[upto, :], low_ref[upto, :]))
        qe_ref[here, :] = grown[here] - mixed[:, :HD]
        o0_ref[here, :] = mixed[:, HD:]


def state_maps(slots, keys, values, write_logits, decays, rates, place, filled):
    length, wide = keys.shape
    heads = wide // HD

    def whose(step, place_ref):
        return 0, head_at(slots, step, place_ref[0], heads)

    column = pl.BlockSpec((length, HD), whose)
    double = pl.BlockSpec((length, 2 * HD), whose)
    table = pl.BlockSpec((heads, length), lambda step, place_ref: (0, 0))
    small = pl.BlockSpec(memory_space=pltpu.SMEM)
    one_map = pl.BlockSpec((HD, 2 * HD), lambda step, place_ref: (0, 0))
    kept = [pl.BlockSpec(memory_space=pl.ANY)] * len(filled)
    return pl.pallas_call(
        functools.partial(maps_kernel, slots),
        grid_spec=pltpu.PrefetchScalarGridSpec(
            num_scalar_prefetch=1,
            grid=(2,),
            in_specs=[small, column, column, table, table, table] + kept,
            out_specs=[one_map, one_map, double, double],
        ),
        out_shape=[pltpu.VMEM((HD, 2 * HD), F32)] * 2
        + [jax.ShapeDtypeStruct((length, 2 * wide), BF16)] * 2,
        input_output_aliases={7: 2, 8: 3} if filled else {},
        name="maps",
    )(place, rates, keys, values, write_logits.T, *decays, *filled)


def mixes(queries, keys, decays, rates, high, low):
    length, wide = queries.shape
    heads = wide // HD
    column = pl.BlockSpec((length, HD), lambda h: (0, h))
    double = pl.BlockSpec((length, 2 * HD), lambda h: (0, h))
    table = pl.BlockSpec((heads, length), lambda h: (0, 0))
    small = pl.BlockSpec(memory_space=pltpu.SMEM)
    return pl.pallas_call(
        mixes_kernel,
        grid=(heads,),
        in_specs=[small, column, column, table, table, double, double],
        out_specs=[column, column],
        out_shape=[jax.ShapeDtypeStruct((length, wide), F32)] * 2,
        name="mixes",
    )(rates, queries, keys, *decays, high, low)


def shift_in(later):
    wide = lax.broadcasted_iota(jnp.int32, later.shape, 1)
    return jnp.where(wide >= HD, later, 0.0)


def then(later, earlier):
    return fine(parts(later[:, :HD]), parts(earlier)) + shift_in(later)


def identity_map():
    ii = lax.broadcasted_iota(jnp.int32, (HD, 2 * HD), 0)
    jj = lax.broadcasted_iota(jnp.int32, (HD, 2 * HD), 1)
    return (ii == jj).astype(F32)


def in_order(place, refs, held_ref):
    number = len(refs)
    for s, ref in enumerate(refs):
        held_ref[(place + number - s) % number] = ref[...]


def all_before_kernel(place_ref, *refs):
    maps, (before_ref, total_ref, held_ref) = refs[:-3], refs[-3:]
    in_order(place_ref[0], maps, held_ref)
    running = identity_map()
    for k in range(len(maps)):
        before_ref[k] = running
        running = held_ref[k] if k == 0 else then(held_ref[k], running)
    total_ref[...] = running


def mine_before_kernel(place_ref, *refs):
    maps, (before_ref, total_ref, held_ref) = refs[:-3], refs[-3:]
    place = place_ref[0]
    in_order(place, maps, held_ref)
    running = identity_map()
    before_ref[...] = running
    for k in range(len(maps)):
        running = held_ref[k] if k == 0 else then(held_ref[k], running)

        @pl.when(place == k + 1)
        def _(running=running):
            before_ref[...] = running

    total_ref[...] = running


def small_call(kernel, out_shape, scratch, place, *arrays):
    return pl.pallas_call(
        kernel,
        in_specs=[pl.BlockSpec(memory_space=pltpu.SMEM)]
        + [pl.BlockSpec(memory_space=pltpu.VMEM)] * len(arrays),
        out_shape=out_shape,
        scratch_shapes=scratch,
        compiler_params=pltpu.CompilerParams(vmem_limit_bytes=8 << 20),
    )(place, *[pltpu.with_memory_space_constraint(a, pltpu.VMEM) for a in arrays])


def states_kernel(place_ref, one_ref, two_ref, three_ref, middle_ref, inner_ref, *out_refs):
    state = three_ref[:, HD:]
    for ref in (two_ref, one_ref, middle_ref):
        state = fine(parts(ref[:, :HD]), parts(state)) + ref[:, HD:]
    pair = parts(state)
    number = len(out_refs)
    for s, out_ref in enumerate(out_refs):
        k = (place_ref[0] + number - s) % number
        out_ref[...] = fine(parts(inner_ref[k, :, :HD]), pair) + inner_ref[k, :, HD:]


def ring(array, axis, step):
    count = lax.axis_size(axis)
    return lax.ppermute(array, axis, [(i, (i + step) % count) for i in range(count)])


def onward(array, axis, step):
    count = lax.axis_size(axis)
    return lax.ppermute(array, axis, [(i, i + step) for i in range(count - step)])


def place_on(axis):
    return lax.axis_index(axis).reshape(1).astype(jnp.int32)


def entering(own, arrived, place):
    number = 1 + len(arrived)
    one = pltpu.VMEM(own.shape, F32)
    many = pltpu.VMEM((number,) + own.shape, F32)
    held = [pltpu.VMEM((number,) + own.shape, F32)]
    inner, line = small_call(all_before_kernel, [many, one], held, place, own, *arrived)
    two = ring(line, "sp_1", 2)
    first, three = [ring(line, "sp_1", s) for s in (1, 3)]
    middle, plane = small_call(
        mine_before_kernel, [one, one], held, place_on("sp_1"), line, first, two, three
    )
    two, first, three = [onward(plane, "sp_0", s) for s in (2, 1, 3)]
    found = small_call(
        states_kernel,
        [pltpu.VMEM((HD, HD), F32)] * number,
        (),
        place,
        first,
        two,
        three,
        middle,
        inner,
    )
    two, first, three = [ring(found[s], "sp_2", number - s) for s in (2, 1, 3)]
    return [found[0], first, two, three]


def finish_kernel(place_ref, core_ref, gain_ref, *refs):
    states, refs = refs[:-10], refs[-10:]
    qe_hbm, o0_hbm, gate_hbm, keep_ref, send_ref, qe_ref, o0_ref, gate_ref, whole_ref, done = refs
    number = len(states)
    half = keep_ref.shape[0]
    core = core_ref[0]
    pairs = ((qe_hbm, qe_ref), (o0_hbm, o0_ref), (gate_hbm, gate_ref))

    def arrival(i, h):
        there = pl.ds(pl.multiple_of(h * HD, HD), HD)
        source, target = pairs[i]
        return pltpu.make_async_copy(source.at[:, there], target.at[:, there], done.at[i, h])

    for h in range(number):
        for i in range(len(pairs)):
            arrival(i, h).start()

    @pl.loop(0, number)
    def _(h):
        there = pl.ds(pl.multiple_of(h * HD, HD), HD)
        slot = (h + number - place_ref[0]) % number
        state = states[0][...]
        for s in range(1, number):
            state = jnp.where(slot == s, states[s][...], state)
        for i in range(len(pairs)):
            arrival(i, h).wait()
        mix = o0_ref[:, there] + fine(parts(qe_ref[:, there]), parts(state))
        scaled = mix * lax.rsqrt(jnp.mean(mix * mix, axis=-1, keepdims=True) + EPS)
        gate = gate_ref[:, there].astype(F32)
        whole_ref[...] = scaled * gain_ref[...] * (gate * jax.nn.sigmoid(gate))
        keep_ref[:, there] = whole_ref[pl.ds(core * half, half), :].astype(BF16)
        send_ref[:, there] = whole_ref[pl.ds((1 - core) * half, half), :].astype(BF16)


def finish(qe, o0, states, gate, gain, place):
    length, wide = gate.shape
    small = pl.BlockSpec(memory_space=pltpu.SMEM)
    arrays = (gain.reshape(1, HD), *states)
    return pl.pallas_call(
        finish_kernel,
        in_specs=[small, small]
        + [pl.BlockSpec(memory_space=pltpu.VMEM)] * len(arrays)
        + [pl.BlockSpec(memory_space=pl.ANY)] * 3,
        out_shape=[pltpu.VMEM((length // 2, wide), BF16)] * 2,
        scratch_shapes=[
            pltpu.VMEM((length, wide), F32),
            pltpu.VMEM((length, wide), F32),
            pltpu.VMEM((length, wide), BF16),
            pltpu.VMEM((length, HD), F32),
            pltpu.SemaphoreType.DMA((3, len(states))),
        ],
        compiler_params=pltpu.CompilerParams(vmem_limit_bytes=12 << 20),
        name="finish",
    )(
        place,
        place_on("tp"),
        *[pltpu.with_memory_space_constraint(a, pltpu.VMEM) for a in arrays],
        *[pltpu.with_memory_space_constraint(a, pltpu.HBM) for a in (qe, o0, gate)],
    )


def feed_forward(rows, w_gate, w_up, w_down):
    hidden = jax.nn.silu(jnp.dot(rows, w_gate, preferred_element_type=F32))
    hidden = (hidden * jnp.dot(rows, w_up, preferred_element_type=F32)).astype(BF16)
    return jnp.dot(hidden, w_down, preferred_element_type=F32)


def exchange(rows):
    return lax.all_to_all(rows, SP_TP, split_axis=0, concat_axis=0, tiled=True)


def routes(index, weight, experts, room):
    length = index.shape[0]
    ids = jnp.arange(experts, dtype=jnp.int32)[:, None]
    named = jnp.zeros((experts, length), F32)
    weights = jnp.zeros((experts, length), F32)
    for j in range(index.shape[1]):
        here = index[:, j][None, :] == ids
        named = named + here.astype(F32)
        weights = weights + jnp.where(here, weight[:, j][None, :], 0.0)
    place = jnp.arange(length, dtype=jnp.int32)
    earlier = (place[:, None] < place[None, :]).astype(BF16)
    slot = jnp.dot(named.astype(BF16), earlier, preferred_element_type=F32)
    plain = jnp.where(named > 0, slot, -1.0)
    slot = plain[:, None, :]
    step = jnp.arange(KEEP, dtype=jnp.int32)[None, :, None]
    extra = room - KEEP
    first = slot == step.astype(F32)
    rest = slot == (KEEP + step % extra).astype(F32)
    lead = rest & (step < extra)
    tail = rest & (step >= extra)
    weights = weights[:, None, :]

    def flat(mask):
        return mask.reshape(experts * KEEP, length)

    back = [flat(jnp.where(m, weights, 0.0).astype(BF16)) for m in (first, lead, tail)]
    return plain, back


def places(slot_ref, start, count, length):
    slot = slot_ref[pl.ds(start, count), :]
    slot = jnp.broadcast_to(slot[:, None, :], (count, KEEP, length)).reshape(count * KEEP, length)
    step = lax.broadcasted_iota(jnp.int32, (count * KEEP, length), 0) % KEEP
    return slot, step


def attend_kernel(
    core_ref, keep_ref, came_ref, gain_ref, slot_ref, matrix_ref, residual_ref, *refs
):
    attended_hbm, normed_hbm, rest_hbm, attended_ref, normed_ref, rest_ref = refs[:6]
    wide_ref, matrix_vmem, residual_vmem, done, gone = refs[6:]
    length, dim = residual_ref.shape
    wide = keep_ref.shape[1]
    number = 4
    block = dim // number
    copies = [pltpu.make_async_copy(residual_ref, residual_vmem, done.at[number])]
    for c in range(number):
        there = pl.ds(c * block, block)
        copies.append(
            pltpu.make_async_copy(matrix_ref.at[:, there], matrix_vmem.at[:, there], done.at[c])
        )
    for copy in copies:
        copy.start()
    keep, came = keep_ref[...].astype(F32), came_ref[...].astype(F32)
    first_core = core_ref[0] == 0
    lead = jnp.where(first_core, keep, came).astype(BF16)
    tail = jnp.where(first_core, came, keep).astype(BF16)
    copies[0].wait()
    squares = jnp.zeros((length, 1), F32)
    for c in range(number):
        there = slice(c * block, (c + 1) * block)
        copies[1 + c].wait()
        projected = dot_nn(lead, matrix_vmem[:wide, there]) + dot_nn(tail, matrix_vmem[wide:, there])
        attended = (residual_vmem[:, there].astype(F32) + projected).astype(BF16)
        attended_ref[:, there] = attended
        plain = attended.astype(F32)
        wide_ref[:, there] = plain
        squares = squares + jnp.sum(plain * plain, axis=-1, keepdims=True)
    leaving = [pltpu.make_async_copy(attended_ref, attended_hbm, gone.at[0])]
    leaving[0].start()
    scale = lax.rsqrt(squares / dim + EPS)
    normed_ref[...] = (wide_ref[...] * scale * gain_ref[...]).astype(BF16)
    leaving.append(pltpu.make_async_copy(normed_ref, normed_hbm, gone.at[1]))
    leaving[1].start()
    half = dim // 2
    count = 32

    def departure(i):
        there = pl.ds(pl.multiple_of(i * count, count), count)
        return pltpu.make_async_copy(rest_ref.at[there], rest_hbm.at[there], gone.at[2 + i])

    @pl.loop(0, slot_ref.shape[0] // count)
    def _(i):
        start = pl.multiple_of(i * count, count)
        slot, step = places(slot_ref, start, count, length)
        extra = KEEP // 2
        chosen = slot == (KEEP + step % extra).astype(F32)
        lead = (chosen & (step < extra)).astype(F32).astype(BF16)
        tail = (chosen & (step >= extra)).astype(F32).astype(BF16)
        rows = dot_nn(lead, normed_ref[:, :half]) + dot_nn(tail, normed_ref[:, half:])
        rest_ref[pl.ds(start, count), :, :] = rows.astype(BF16).reshape(count, KEEP, half)
        departure(i).start()

    for i in range(slot_ref.shape[0] // count):
        departure(i).wait()
    for copy in leaving:
        copy.wait()


def attend(keep, came, out_matrix, residual, gain, slot):
    length, dim = residual.shape
    experts = slot.shape[0]
    arrays = (keep, came, gain.reshape(1, dim), slot)
    rows = pltpu.HBM((length, dim), BF16)
    return pl.pallas_call(
        attend_kernel,
        in_specs=[pl.BlockSpec(memory_space=pltpu.SMEM)]
        + [pl.BlockSpec(memory_space=pltpu.VMEM)] * len(arrays)
        + [pl.BlockSpec(memory_space=pl.ANY)] * 2,
        out_specs=[pl.BlockSpec(memory_space=pl.ANY)] * 3,
        out_shape=[rows, rows, pltpu.HBM((experts, KEEP, dim // 2), BF16)],
        scratch_shapes=[
            pltpu.VMEM((length, dim), BF16),
            pltpu.VMEM((length, dim), BF16),
            pltpu.VMEM((experts, KEEP, dim // 2), BF16),
            pltpu.VMEM((length, dim), F32),
            pltpu.VMEM(out_matrix.shape, BF16),
            pltpu.VMEM((length, dim), BF16),
            pltpu.SemaphoreType.DMA((5,)),
            pltpu.SemaphoreType.DMA((2 + experts // 32,)),
        ],
        name="attend",
    )(
        place_on("tp"),
        *[pltpu.with_memory_space_constraint(a, pltpu.VMEM) for a in arrays],
        *[pltpu.with_memory_space_constraint(a, pltpu.HBM) for a in (out_matrix, residual)],
    )


def dispatch_kernel(slot_ref, normed_ref, out_ref):
    count, _, dim = out_ref.shape
    start = pl.multiple_of(pl.program_id(0) * count, count)
    slot, step = places(slot_ref, start, count, normed_ref.shape[0])
    chosen = (slot == step.astype(F32)).astype(F32).astype(BF16)
    rows = dot_nn(chosen, normed_ref[...]).astype(BF16)
    out_ref[...] = rows.reshape(count, KEEP, dim)


def dispatch(slot, normed):
    experts, length = slot.shape
    dim = normed.shape[1]
    count = 16
    return pl.pallas_call(
        dispatch_kernel,
        grid=(experts // count,),
        in_specs=[
            pl.BlockSpec((experts, length), lambda i: (0, 0)),
            pl.BlockSpec((length, dim), lambda i: (0, 0)),
        ],
        out_specs=pl.BlockSpec((count, KEEP, dim), lambda i: (i, 0, 0)),
        out_shape=jax.ShapeDtypeStruct((experts, KEEP, dim), BF16),
        name="dispatch",
    )(slot, normed)


def final_kernel(table_ref, early_ref, rows_ref, out_ref, early_vmem, rows_vmem, out_vmem, done):
    number = done.shape[1]
    block = out_vmem.shape[1] // number
    spans = [pl.ds(c * block, block) for c in range(number)]
    comes = [
        pltpu.make_async_copy(rows_ref.at[:, s], rows_vmem.at[:, s], done.at[0, c])
        for c, s in enumerate(spans)
    ]
    goes = [
        pltpu.make_async_copy(out_vmem.at[:, s], out_ref.at[:, s], done.at[1, c])
        for c, s in enumerate(spans)
    ]
    sums = [
        pltpu.make_async_copy(early_ref.at[:, s], early_vmem.at[:, s], done.at[2, c])
        for c, s in enumerate(spans)
    ]
    for c in range(number):
        comes[c].start()
        sums[c].start()
    for c in range(number):
        there = slice(c * block, (c + 1) * block)
        comes[c].wait()
        sums[c].wait()
        total = early_vmem[:, there] + dot_nn(table_ref[...], rows_vmem[:, there])
        out_vmem[:, there] = total.astype(BF16)
        goes[c].start()
    for copy in goes:
        copy.wait()


def final_sum(table, rows, early):
    length, wide = early.shape
    return pl.pallas_call(
        final_kernel,
        in_specs=[pl.BlockSpec(memory_space=pltpu.VMEM)] + [pl.BlockSpec(memory_space=pl.ANY)] * 2,
        out_specs=pl.BlockSpec(memory_space=pl.ANY),
        out_shape=pltpu.HBM((length, wide), BF16),
        scratch_shapes=[
            pltpu.VMEM((length, wide), F32),
            pltpu.VMEM(rows.shape, BF16),
            pltpu.VMEM((length, wide), BF16),
            pltpu.SemaphoreType.DMA((3, 4)),
        ],
        compiler_params=pltpu.CompilerParams(vmem_limit_bytes=16 << 20),
        name="final_sum",
    )(
        pltpu.with_memory_space_constraint(table, pltpu.VMEM),
        *[pltpu.with_memory_space_constraint(a, pltpu.HBM) for a in (early, rows)],
    )


def shards(
    projected_queries,
    projected_keys,
    projected_values,
    output_gate_values,
    write_strength_logits,
    decay_input_logits,
    head_rate_logarithm,
    extra_log_decay,
    per_head_norm_gain,
    output_matrix,
    residual,
    mixture_norm_gain,
    selected_expert_index,
    routing_weight,
    routed_gate_weight,
    routed_up_weight,
    routed_down_weight,
    common_gate_weight,
    common_up_weight,
    common_down_weight,
):
    place = place_on("sp_2")
    decays = (decay_input_logits.T, extra_log_decay.T)
    base = (projected_keys, projected_values, write_strength_logits, decays, head_rate_logarithm)
    far, near, high, low = state_maps((2, 1), *base, place, ())
    far = ring(far, "sp_2", 2)
    near = ring(near, "sp_2", 1)
    last, own, high, low = state_maps((3, 0), *base, place, (high, low))
    states = entering(own, (near, far, ring(last, "sp_2", 3)), place)
    qe, o0 = mixes(projected_queries, projected_keys, decays, head_rate_logarithm, high, low)
    keep, send = finish(qe, o0, states, output_gate_values, per_head_norm_gain, place)
    came = ring(send, "tp", 1)
    length, dim = residual.shape
    experts = lax.axis_size(SP) * lax.axis_size("tp")
    room = max(2, length * TOP_K * 3 // (2 * experts))
    extra = room - KEEP
    half = dim // 2
    slot, (w_first, w_lead, w_tail) = routes(selected_expert_index, routing_weight, experts, room)
    attended, normed, rest_out = attend(
        keep, came, output_matrix, residual, mixture_norm_gain, slot
    )
    rest_in = exchange(rest_out)
    main_in = exchange(dispatch(slot, normed))
    shared = feed_forward(normed, common_gate_weight, common_up_weight, common_down_weight)

    weights = (routed_gate_weight[0], routed_up_weight[0], routed_down_weight[0])
    main_rows = feed_forward(main_in.reshape(experts * KEEP, dim), *weights).astype(BF16)
    main_back = exchange(main_rows.reshape(experts, KEEP, dim)).reshape(experts * KEEP, dim)
    unfolded = rest_in.reshape(experts, 2, extra, half).transpose(0, 2, 1, 3)
    rest_rows = feed_forward(unfolded.reshape(experts * extra, dim), *weights).astype(BF16)
    folded = rest_rows.reshape(experts, extra, 2, half).transpose(0, 2, 1, 3)
    rest_back = exchange(folded.reshape(experts, KEEP, half)).reshape(experts * KEEP, half)

    def combine(table, rows):
        return lax.dot_general(table, rows, (((0,), (0,)), ((), ())), preferred_element_type=F32)

    early = jnp.concatenate([combine(w_lead, rest_back), combine(w_tail, rest_back)], axis=1)
    early = early + attended.astype(F32) + shared
    return final_sum(w_first.T, main_back, early)


def solution(mesh):
    finer = Mesh(mesh.devices.reshape(4, 4, 4, mesh.shape["tp"]), ("sp_0", "sp_1", "sp_2", "tp"))
    in_specs = (
        P(SP, "tp"),
        P(SP, "tp"),
        P(SP, "tp"),
        P(SP, "tp"),
        P(SP, "tp"),
        P(SP, "tp"),
        P("tp"),
        P(SP, "tp"),
        P(),
        P(),
        P(SP_TP, None),
        P(),
        P(SP_TP, None),
        P(SP_TP, None),
        P(SP_TP, None, None),
        P(SP_TP, None, None),
        P(SP_TP, None, None),
        P(),
        P(),
        P(),
    )
    out_specs = P(SP_TP, None)

    return jax.shard_map(
        shards, mesh=finer, in_specs=in_specs, out_specs=out_specs, check_vma=False
    )
```

```python
import jax
import jax.numpy as jnp
from jax import lax
from jax.experimental import pallas as pl
from jax.experimental.pallas import tpu as pltpu
from jax.sharding import Mesh
from jax.sharding import PartitionSpec as P

TOP_K = 4
HD = 128
BLOCK = 128
KEEP = 8
SP = ("sp_0", "sp_1", "sp_2")
SP_TP = ("sp_0", "sp_1", "sp_2", "tp")
EPS = 1e-06
F32 = jnp.float32
BF16 = jnp.bfloat16


def dot_nn(a, b):
    return lax.dot_general(a, b, (((1,), (0,)), ((), ())), preferred_element_type=F32)


def dot_nt(a, b):
    return lax.dot_general(a, b, (((1,), (1,)), ((), ())), preferred_element_type=F32)


def dot_tn(a, b):
    return lax.dot_general(a, b, (((0,), (0,)), ((), ())), preferred_element_type=F32)


def parts(x):
    high = x.astype(BF16)
    return high, (x - high.astype(F32)).astype(BF16)


def rows_of(*arrays):
    return jnp.concatenate(arrays, axis=0)


def cols_of(*arrays):
    return jnp.concatenate(arrays, axis=1)


def fine(a, b):
    ah, al = a
    bh, bl = b
    return dot_nn(cols_of(ah, al), rows_of(bh, bh)) + dot_nn(ah, bl)


def fine_square(a, b):
    ah, al = a
    bh, bl = b
    both = dot_nn(cols_of(ah, al), rows_of(cols_of(bh, bl), cols_of(bh, jnp.zeros_like(bl))))
    return both[:, :HD] + both[:, HD:]


def own_row(ref, head):
    table = ref[...].astype(F32)
    which = lax.broadcasted_iota(jnp.int32, table.shape, 0)
    return jnp.sum(jnp.where(which == head, table, 0.0), axis=0, keepdims=True)


def decay_sums(rate_ref, decay_ref, extra_ref, head):
    length = decay_ref.shape[1]
    raw = own_row(decay_ref, head) - 6.0
    soft = jnp.maximum(raw, 0.0) + jnp.log1p(jnp.exp(-jnp.abs(raw)))
    rate = jnp.exp(jnp.full((1, length), rate_ref[head], F32))
    total = jnp.broadcast_to(own_row(extra_ref, head) - rate * soft, (8, length))
    lane = lax.broadcasted_iota(jnp.int32, total.shape, 1)
    shift = 1
    while shift < length:
        total = total + jnp.where(lane >= shift, pltpu.roll(total, shift, 1), 0.0)
        shift *= 2
    g_row = total[0:1, :]
    return g_row, jnp.broadcast_to(g_row, (HD, length)).T


def unit(raw):
    x = raw.astype(F32)
    active = x * jax.nn.sigmoid(x)
    return active * lax.rsqrt(jnp.sum(active * active, axis=-1, keepdims=True) + EPS)


def against_keys(left, keys, number, g_row, g_col):
    ii = lax.broadcasted_iota(jnp.int32, (BLOCK, BLOCK), 0)
    jj = lax.broadcasted_iota(jnp.int32, (BLOCK, BLOCK), 1)
    blocks = []
    for r in range(number):
        here = slice(r * BLOCK, (r + 1) * BLOCK)
        upto = slice(0, (r + 1) * BLOCK)
        high = keys[0][upto]
        both = dot_nt(cols_of(left[0][here], left[1][here]), cols_of(high, high))
        both = both + dot_nt(left[0][here], keys[1][upto])
        row = []
        for c in range(r + 1):
            there = slice(c * BLOCK, (c + 1) * BLOCK)
            gap = g_col[here] - g_row[:, there]
            if c == r:
                gap = jnp.where(ii >= jj, gap, -1e30)
            row.append(both[:, there] * jnp.exp(gap))
        blocks.append(row)
    return blocks


PAIR = 2


def maps_kernel(place_ref, rate_ref, k_ref, v_ref, write_ref, decay_ref, extra_ref, *refs):
    map_refs, (high_ref, low_ref) = refs[:-2], refs[-2:]
    heads = len(map_refs)
    length = k_ref.shape[0]
    number = length // BLOCK
    ii = lax.broadcasted_iota(jnp.int32, (BLOCK, BLOCK), 0)
    jj = lax.broadcasted_iota(jnp.int32, (BLOCK, BLOCK), 1)
    eye = (ii == jj).astype(F32)
    pair = range(PAIR)
    heads_here = [pl.program_id(0) * PAIR + p for p in pair]
    lower, right, late, last = [], [], [], []
    for p in pair:
        there = slice(p * HD, (p + 1) * HD)
        g_row, g_col = decay_sums(rate_ref, decay_ref, extra_ref, heads_here[p])
        beta = jax.nn.sigmoid(own_row(write_ref, heads_here[p]))
        b_col = jnp.broadcast_to(beta, (HD, length)).T
        keys = unit(k_ref[:, there])
        raw = v_ref[:, there].astype(F32)
        values = raw * jax.nn.sigmoid(raw)
        k_beta = keys * b_col
        right.append(cols_of(k_beta * jnp.exp(g_col), values * b_col))
        last.append(g_col[length - 1 : length, :])
        late.append(parts(keys * jnp.exp(last[p] - g_col)))
        lower.append(against_keys(parts(k_beta), parts(keys), number, g_row, g_col))
    near = (ii // 2 == jj // 2) & (ii > jj)
    chains = [(p, r) for r in range(number) for p in pair]
    inverse = {(p, r): eye - jnp.where(near, lower[p][r][r], 0.0) for p, r in chains}
    for level in range(1, BLOCK.bit_length() - 1):
        chosen = (ii >> (level + 1) == jj >> (level + 1)) & (ii >> level > jj >> level)
        halves = {c: parts(inverse[c]) for c in chains}
        steps = {
            (p, r): fine_square(halves[p, r], parts(jnp.where(chosen, lower[p][r][r], 0.0)))
            for p, r in chains
        }
        inverse = {c: inverse[c] - fine_square(parts(steps[c]), halves[c]) for c in chains}
    highs, lows = [[] for _ in pair], [[] for _ in pair]
    for p, r in chains:
        here = slice(r * BLOCK, (r + 1) * BLOCK)
        there = slice(2 * p * HD, 2 * (p + 1) * HD)
        rest = right[p][here]
        if r > 0:
            known = (rows_of(*highs[p]), rows_of(*lows[p]))
            rest = rest - fine(parts(cols_of(*lower[p][r][:r])), known)
        one = parts(fine(parts(inverse[p, r]), parts(rest)))
        highs[p].append(one[0])
        lows[p].append(one[1])
        high_ref[here, there] = one[0]
        low_ref[here, there] = one[1]
    for p in pair:
        high, low = rows_of(*highs[p]), rows_of(*lows[p])
        moved = dot_tn(rows_of(*late[p]), rows_of(high, high)) + dot_tn(late[p][0], low)
        whole = cols_of(eye * jnp.exp(last[p]) - moved[:, :HD], moved[:, HD:])
        slot = (heads_here[p] + heads - place_ref[0]) % heads
        for s, map_ref in enumerate(map_refs):

            @pl.when(slot == s)
            def _(map_ref=map_ref, whole=whole):
                map_ref[...] = whole


def mixes_kernel(rate_ref, q_ref, k_ref, decay_ref, extra_ref, high_ref, low_ref, qe_ref, o0_ref):
    length = q_ref.shape[0]
    number = length // BLOCK
    g_row, g_col = decay_sums(rate_ref, decay_ref, extra_ref, pl.program_id(0))
    queries = unit(q_ref[...])
    mixing = against_keys(parts(queries), parts(unit(k_ref[...])), number, g_row, g_col)
    grown = queries * jnp.exp(g_col)
    for r in range(number):
        here = slice(r * BLOCK, (r + 1) * BLOCK)
        upto = slice(0, (r + 1) * BLOCK)
        mixed = fine(parts(cols_of(*mixing[r])), (high_ref[upto, :], low_ref[upto, :]))
        qe_ref[here, :] = grown[here] - mixed[:, :HD]
        o0_ref[here, :] = mixed[:, HD:]


def state_maps(keys, values, write_logits, decays, rates, place):
    length, wide = keys.shape
    heads = wide // HD
    column = pl.BlockSpec((length, PAIR * HD), lambda step: (0, step))
    double = pl.BlockSpec((length, 2 * PAIR * HD), lambda step: (0, step))
    table = pl.BlockSpec((heads, length), lambda step: (0, 0))
    small = pl.BlockSpec(memory_space=pltpu.SMEM)
    one_map = pl.BlockSpec((HD, 2 * HD), lambda step: (0, 0))
    out = pl.pallas_call(
        maps_kernel,
        grid=(heads // PAIR,),
        in_specs=[small, small, column, column, table, table, table],
        out_specs=[one_map] * heads + [double, double],
        out_shape=[pltpu.VMEM((HD, 2 * HD), F32)] * heads
        + [jax.ShapeDtypeStruct((length, 2 * wide), BF16)] * 2,
        name="maps",
    )(place, rates, keys, values, write_logits.T, *decays)
    return out[:heads], out[heads], out[heads + 1]


def mixes(queries, keys, decays, rates, high, low):
    length, wide = queries.shape
    heads = wide // HD
    column = pl.BlockSpec((length, HD), lambda h: (0, h))
    double = pl.BlockSpec((length, 2 * HD), lambda h: (0, h))
    table = pl.BlockSpec((heads, length), lambda h: (0, 0))
    small = pl.BlockSpec(memory_space=pltpu.SMEM)
    return pl.pallas_call(
        mixes_kernel,
        grid=(heads,),
        in_specs=[small, column, column, table, table, double, double],
        out_specs=[column, column],
        out_shape=[jax.ShapeDtypeStruct((length, wide), F32)] * 2,
        name="mixes",
    )(rates, queries, keys, *decays, high, low)


def shift_in(later):
    wide = lax.broadcasted_iota(jnp.int32, later.shape, 1)
    return jnp.where(wide >= HD, later, 0.0)


def then(later, earlier):
    return fine(parts(later[:, :HD]), parts(earlier)) + shift_in(later)


def identity_map():
    ii = lax.broadcasted_iota(jnp.int32, (HD, 2 * HD), 0)
    jj = lax.broadcasted_iota(jnp.int32, (HD, 2 * HD), 1)
    return (ii == jj).astype(F32)


def in_order(place, refs, held_ref):
    number = len(refs)
    for s, ref in enumerate(refs):
        held_ref[(place + number - s) % number] = ref[...]


def all_before_kernel(place_ref, *refs):
    maps, (before_ref, total_ref, held_ref) = refs[:-3], refs[-3:]
    in_order(place_ref[0], maps, held_ref)
    running = identity_map()
    for k in range(len(maps)):
        before_ref[k] = running
        running = held_ref[k] if k == 0 else then(held_ref[k], running)
    total_ref[...] = running


def mine_before_kernel(place_ref, *refs):
    maps, (before_ref, total_ref, held_ref) = refs[:-3], refs[-3:]
    place = place_ref[0]
    in_order(place, maps, held_ref)
    running = identity_map()
    before_ref[...] = running
    for k in range(len(maps)):
        running = held_ref[k] if k == 0 else then(held_ref[k], running)

        @pl.when(place == k + 1)
        def _(running=running):
            before_ref[...] = running

    total_ref[...] = running


def small_call(kernel, out_shape, scratch, place, *arrays):
    return pl.pallas_call(
        kernel,
        in_specs=[pl.BlockSpec(memory_space=pltpu.SMEM)]
        + [pl.BlockSpec(memory_space=pltpu.VMEM)] * len(arrays),
        out_shape=out_shape,
        scratch_shapes=scratch,
        compiler_params=pltpu.CompilerParams(vmem_limit_bytes=8 << 20),
    )(place, *[pltpu.with_memory_space_constraint(a, pltpu.VMEM) for a in arrays])


def states_kernel(place_ref, one_ref, two_ref, three_ref, middle_ref, inner_ref, *out_refs):
    state = three_ref[:, HD:]
    for ref in (two_ref, one_ref, middle_ref):
        state = fine(parts(ref[:, :HD]), parts(state)) + ref[:, HD:]
    pair = parts(state)
    number = len(out_refs)
    for s, out_ref in enumerate(out_refs):
        k = (place_ref[0] + number - s) % number
        out_ref[...] = fine(parts(inner_ref[k, :, :HD]), pair) + inner_ref[k, :, HD:]


def ring(array, axis, step):
    count = lax.axis_size(axis)
    return lax.ppermute(array, axis, [(i, (i + step) % count) for i in range(count)])


def onward(array, axis, step):
    count = lax.axis_size(axis)
    return lax.ppermute(array, axis, [(i, i + step) for i in range(count - step)])


def place_on(axis):
    return lax.axis_index(axis).reshape(1).astype(jnp.int32)


def entering(own, arrived, place):
    number = 1 + len(arrived)
    one = pltpu.VMEM(own.shape, F32)
    many = pltpu.VMEM((number,) + own.shape, F32)
    held = [pltpu.VMEM((number,) + own.shape, F32)]
    inner, line = small_call(all_before_kernel, [many, one], held, place, own, *arrived)
    two, first, three = [ring(line, "sp_1", s) for s in (2, 1, 3)]
    middle, plane = small_call(
        mine_before_kernel, [one, one], held, place_on("sp_1"), line, first, two, three
    )
    two, first, three = [onward(plane, "sp_0", s) for s in (2, 1, 3)]
    found = small_call(
        states_kernel,
        [pltpu.VMEM((HD, HD), F32)] * number,
        (),
        place,
        first,
        two,
        three,
        middle,
        inner,
    )
    two, first, three = [ring(found[s], "sp_2", number - s) for s in (2, 1, 3)]
    return [found[0], first, two, three]


def finish_kernel(place_ref, core_ref, gain_ref, *refs):
    states, refs = refs[:-10], refs[-10:]
    qe_hbm, o0_hbm, gate_hbm, keep_ref, send_ref, qe_ref, o0_ref, gate_ref, whole_ref, done = refs
    number = len(states)
    half = keep_ref.shape[0]
    core = core_ref[0]
    pairs = ((qe_hbm, qe_ref), (o0_hbm, o0_ref), (gate_hbm, gate_ref))

    def arrival(i, h):
        there = pl.ds(pl.multiple_of(h * HD, HD), HD)
        source, target = pairs[i]
        return pltpu.make_async_copy(source.at[:, there], target.at[:, there], done.at[i, h])

    for h in range(number):
        for i in range(len(pairs)):
            arrival(i, h).start()

    @pl.loop(0, number)
    def _(h):
        there = pl.ds(pl.multiple_of(h * HD, HD), HD)
        slot = (h + number - place_ref[0]) % number
        state = states[0][...]
        for s in range(1, number):
            state = jnp.where(slot == s, states[s][...], state)
        for i in range(len(pairs)):
            arrival(i, h).wait()
        mix = o0_ref[:, there] + fine(parts(qe_ref[:, there]), parts(state))
        scaled = mix * lax.rsqrt(jnp.mean(mix * mix, axis=-1, keepdims=True) + EPS)
        gate = gate_ref[:, there].astype(F32)
        whole_ref[...] = scaled * gain_ref[...] * (gate * jax.nn.sigmoid(gate))
        keep_ref[:, there] = whole_ref[pl.ds(core * half, half), :].astype(BF16)
        send_ref[:, there] = whole_ref[pl.ds((1 - core) * half, half), :].astype(BF16)


def finish(qe, o0, states, gate, gain, place):
    length, wide = gate.shape
    small = pl.BlockSpec(memory_space=pltpu.SMEM)
    arrays = (gain.reshape(1, HD), *states)
    return pl.pallas_call(
        finish_kernel,
        in_specs=[small, small]
        + [pl.BlockSpec(memory_space=pltpu.VMEM)] * len(arrays)
        + [pl.BlockSpec(memory_space=pl.ANY)] * 3,
        out_shape=[pltpu.VMEM((length // 2, wide), BF16)] * 2,
        scratch_shapes=[
            pltpu.VMEM((length, wide), F32),
            pltpu.VMEM((length, wide), F32),
            pltpu.VMEM((length, wide), BF16),
            pltpu.VMEM((length, HD), F32),
            pltpu.SemaphoreType.DMA((3, len(states))),
        ],
        compiler_params=pltpu.CompilerParams(vmem_limit_bytes=12 << 20),
        name="finish",
    )(
        place,
        place_on("tp"),
        *[pltpu.with_memory_space_constraint(a, pltpu.VMEM) for a in arrays],
        *[pltpu.with_memory_space_constraint(a, pltpu.HBM) for a in (qe, o0, gate)],
    )


def feed_forward(rows, w_gate, w_up, w_down):
    hidden = jax.nn.silu(jnp.dot(rows, w_gate, preferred_element_type=F32))
    hidden = (hidden * jnp.dot(rows, w_up, preferred_element_type=F32)).astype(BF16)
    return jnp.dot(hidden, w_down, preferred_element_type=F32)


def exchange(rows):
    return lax.all_to_all(rows, SP_TP, split_axis=0, concat_axis=0, tiled=True)


def routes(index, weight, experts, room):
    length = index.shape[0]
    ids = jnp.arange(experts, dtype=jnp.int32)[:, None]
    named = jnp.zeros((experts, length), F32)
    weights = jnp.zeros((experts, length), F32)
    for j in range(index.shape[1]):
        here = index[:, j][None, :] == ids
        named = named + here.astype(F32)
        weights = weights + jnp.where(here, weight[:, j][None, :], 0.0)
    place = jnp.arange(length, dtype=jnp.int32)
    earlier = (place[:, None] < place[None, :]).astype(BF16)
    slot = jnp.dot(named.astype(BF16), earlier, preferred_element_type=F32)
    plain = jnp.where(named > 0, slot, -1.0)
    slot = plain[:, None, :]
    step = jnp.arange(KEEP, dtype=jnp.int32)[None, :, None]
    extra = room - KEEP
    first = slot == step.astype(F32)
    rest = slot == (KEEP + step % extra).astype(F32)
    lead = rest & (step < extra)
    tail = rest & (step >= extra)
    weights = weights[:, None, :]

    def flat(mask):
        return mask.reshape(experts * KEEP, length)

    back = [flat(jnp.where(m, weights, 0.0).astype(BF16)) for m in (first, lead, tail)]
    return plain, back


def places(slot_ref, start, count, length):
    slot = slot_ref[pl.ds(start, count), :]
    slot = jnp.broadcast_to(slot[:, None, :], (count, KEEP, length)).reshape(count * KEEP, length)
    step = lax.broadcasted_iota(jnp.int32, (count * KEEP, length), 0) % KEEP
    return slot, step


def attend_kernel(
    core_ref, keep_ref, came_ref, gain_ref, slot_ref, matrix_ref, residual_ref, *refs
):
    attended_hbm, normed_hbm, rest_hbm, attended_ref, normed_ref, rest_ref = refs[:6]
    wide_ref, matrix_vmem, residual_vmem, done, gone = refs[6:]
    length, dim = residual_ref.shape
    wide = keep_ref.shape[1]
    number = 4
    block = dim // number
    copies = [pltpu.make_async_copy(residual_ref, residual_vmem, done.at[number])]
    for c in range(number):
        there = pl.ds(c * block, block)
        copies.append(
            pltpu.make_async_copy(matrix_ref.at[:, there], matrix_vmem.at[:, there], done.at[c])
        )
    for copy in copies:
        copy.start()
    keep, came = keep_ref[...].astype(F32), came_ref[...].astype(F32)
    first_core = core_ref[0] == 0
    lead = jnp.where(first_core, keep, came).astype(BF16)
    tail = jnp.where(first_core, came, keep).astype(BF16)
    copies[0].wait()
    squares = jnp.zeros((length, 1), F32)
    for c in range(number):
        there = slice(c * block, (c + 1) * block)
        copies[1 + c].wait()
        projected = dot_nn(lead, matrix_vmem[:wide, there]) + dot_nn(tail, matrix_vmem[wide:, there])
        attended = (residual_vmem[:, there].astype(F32) + projected).astype(BF16)
        attended_ref[:, there] = attended
        plain = attended.astype(F32)
        wide_ref[:, there] = plain
        squares = squares + jnp.sum(plain * plain, axis=-1, keepdims=True)
    leaving = [pltpu.make_async_copy(attended_ref, attended_hbm, gone.at[0])]
    leaving[0].start()
    scale = lax.rsqrt(squares / dim + EPS)
    normed_ref[...] = (wide_ref[...] * scale * gain_ref[...]).astype(BF16)
    leaving.append(pltpu.make_async_copy(normed_ref, normed_hbm, gone.at[1]))
    leaving[1].start()
    half = dim // 2
    count = 32

    def departure(i):
        there = pl.ds(pl.multiple_of(i * count, count), count)
        return pltpu.make_async_copy(rest_ref.at[there], rest_hbm.at[there], gone.at[2 + i])

    @pl.loop(0, slot_ref.shape[0] // count)
    def _(i):
        start = pl.multiple_of(i * count, count)
        slot, step = places(slot_ref, start, count, length)
        extra = KEEP // 2
        chosen = slot == (KEEP + step % extra).astype(F32)
        lead = (chosen & (step < extra)).astype(F32).astype(BF16)
        tail = (chosen & (step >= extra)).astype(F32).astype(BF16)
        rows = dot_nn(lead, normed_ref[:, :half]) + dot_nn(tail, normed_ref[:, half:])
        rest_ref[pl.ds(start, count), :, :] = rows.astype(BF16).reshape(count, KEEP, half)
        departure(i).start()

    for i in range(slot_ref.shape[0] // count):
        departure(i).wait()
    for copy in leaving:
        copy.wait()


def attend(keep, came, out_matrix, residual, gain, slot):
    length, dim = residual.shape
    experts = slot.shape[0]
    arrays = (keep, came, gain.reshape(1, dim), slot)
    rows = pltpu.HBM((length, dim), BF16)
    return pl.pallas_call(
        attend_kernel,
        in_specs=[pl.BlockSpec(memory_space=pltpu.SMEM)]
        + [pl.BlockSpec(memory_space=pltpu.VMEM)] * len(arrays)
        + [pl.BlockSpec(memory_space=pl.ANY)] * 2,
        out_specs=[pl.BlockSpec(memory_space=pl.ANY)] * 3,
        out_shape=[rows, rows, pltpu.HBM((experts, KEEP, dim // 2), BF16)],
        scratch_shapes=[
            pltpu.VMEM((length, dim), BF16),
            pltpu.VMEM((length, dim), BF16),
            pltpu.VMEM((experts, KEEP, dim // 2), BF16),
            pltpu.VMEM((length, dim), F32),
            pltpu.VMEM(out_matrix.shape, BF16),
            pltpu.VMEM((length, dim), BF16),
            pltpu.SemaphoreType.DMA((5,)),
            pltpu.SemaphoreType.DMA((2 + experts // 32,)),
        ],
        name="attend",
    )(
        place_on("tp"),
        *[pltpu.with_memory_space_constraint(a, pltpu.VMEM) for a in arrays],
        *[pltpu.with_memory_space_constraint(a, pltpu.HBM) for a in (out_matrix, residual)],
    )


def dispatch_kernel(slot_ref, normed_ref, out_ref):
    count, _, dim = out_ref.shape
    start = pl.multiple_of(pl.program_id(0) * count, count)
    slot, step = places(slot_ref, start, count, normed_ref.shape[0])
    chosen = (slot == step.astype(F32)).astype(F32).astype(BF16)
    rows = dot_nn(chosen, normed_ref[...]).astype(BF16)
    out_ref[...] = rows.reshape(count, KEEP, dim)


def dispatch(slot, normed):
    experts, length = slot.shape
    dim = normed.shape[1]
    count = 16
    return pl.pallas_call(
        dispatch_kernel,
        grid=(experts // count,),
        in_specs=[
            pl.BlockSpec((experts, length), lambda i: (0, 0)),
            pl.BlockSpec((length, dim), lambda i: (0, 0)),
        ],
        out_specs=pl.BlockSpec((count, KEEP, dim), lambda i: (i, 0, 0)),
        out_shape=jax.ShapeDtypeStruct((experts, KEEP, dim), BF16),
        name="dispatch",
    )(slot, normed)


def final_kernel(table_ref, early_ref, rows_ref, out_ref, early_vmem, rows_vmem, out_vmem, done):
    number = done.shape[1]
    block = out_vmem.shape[1] // number
    spans = [pl.ds(c * block, block) for c in range(number)]
    comes = [
        pltpu.make_async_copy(rows_ref.at[:, s], rows_vmem.at[:, s], done.at[0, c])
        for c, s in enumerate(spans)
    ]
    goes = [
        pltpu.make_async_copy(out_vmem.at[:, s], out_ref.at[:, s], done.at[1, c])
        for c, s in enumerate(spans)
    ]
    sums = [
        pltpu.make_async_copy(early_ref.at[:, s], early_vmem.at[:, s], done.at[2, c])
        for c, s in enumerate(spans)
    ]
    for c in range(number):
        comes[c].start()
        sums[c].start()
    for c in range(number):
        there = slice(c * block, (c + 1) * block)
        comes[c].wait()
        sums[c].wait()
        total = early_vmem[:, there] + dot_nn(table_ref[...], rows_vmem[:, there])
        out_vmem[:, there] = total.astype(BF16)
        goes[c].start()
    for copy in goes:
        copy.wait()


def final_sum(table, rows, early):
    length, wide = early.shape
    return pl.pallas_call(
        final_kernel,
        in_specs=[pl.BlockSpec(memory_space=pltpu.VMEM)] + [pl.BlockSpec(memory_space=pl.ANY)] * 2,
        out_specs=pl.BlockSpec(memory_space=pl.ANY),
        out_shape=pltpu.HBM((length, wide), BF16),
        scratch_shapes=[
            pltpu.VMEM((length, wide), F32),
            pltpu.VMEM(rows.shape, BF16),
            pltpu.VMEM((length, wide), BF16),
            pltpu.SemaphoreType.DMA((3, 4)),
        ],
        compiler_params=pltpu.CompilerParams(vmem_limit_bytes=16 << 20),
        name="final_sum",
    )(
        pltpu.with_memory_space_constraint(table, pltpu.VMEM),
        *[pltpu.with_memory_space_constraint(a, pltpu.HBM) for a in (early, rows)],
    )


def shards(
    projected_queries,
    projected_keys,
    projected_values,
    output_gate_values,
    write_strength_logits,
    decay_input_logits,
    head_rate_logarithm,
    extra_log_decay,
    per_head_norm_gain,
    output_matrix,
    residual,
    mixture_norm_gain,
    selected_expert_index,
    routing_weight,
    routed_gate_weight,
    routed_up_weight,
    routed_down_weight,
    common_gate_weight,
    common_up_weight,
    common_down_weight,
):
    place = place_on("sp_2")
    decays = (decay_input_logits.T, extra_log_decay.T)
    (own, near, far, last), high, low = state_maps(
        projected_keys,
        projected_values,
        write_strength_logits,
        decays,
        head_rate_logarithm,
        place,
    )
    far = ring(far, "sp_2", 2)
    near, last = ring(near, "sp_2", 1), ring(last, "sp_2", 3)
    states = entering(own, (near, far, last), place)
    qe, o0 = mixes(projected_queries, projected_keys, decays, head_rate_logarithm, high, low)
    keep, send = finish(qe, o0, states, output_gate_values, per_head_norm_gain, place)
    came = ring(send, "tp", 1)
    length, dim = residual.shape
    experts = lax.axis_size(SP) * lax.axis_size("tp")
    room = max(2, length * TOP_K * 3 // (2 * experts))
    extra = room - KEEP
    half = dim // 2
    slot, (w_first, w_lead, w_tail) = routes(selected_expert_index, routing_weight, experts, room)
    attended, normed, rest_out = attend(
        keep, came, output_matrix, residual, mixture_norm_gain, slot
    )
    rest_in = exchange(rest_out)
    main_in = exchange(dispatch(slot, normed))
    shared = feed_forward(normed, common_gate_weight, common_up_weight, common_down_weight)

    weights = (routed_gate_weight[0], routed_up_weight[0], routed_down_weight[0])
    main_rows = feed_forward(main_in.reshape(experts * KEEP, dim), *weights).astype(BF16)
    main_back = exchange(main_rows.reshape(experts, KEEP, dim)).reshape(experts * KEEP, dim)
    unfolded = rest_in.reshape(experts, 2, extra, half).transpose(0, 2, 1, 3)
    rest_rows = feed_forward(unfolded.reshape(experts * extra, dim), *weights).astype(BF16)
    folded = rest_rows.reshape(experts, extra, 2, half).transpose(0, 2, 1, 3)
    rest_back = exchange(folded.reshape(experts, KEEP, half)).reshape(experts * KEEP, half)

    def combine(table, rows):
        return lax.dot_general(table, rows, (((0,), (0,)), ((), ())), preferred_element_type=F32)

    early = jnp.concatenate([combine(w_lead, rest_back), combine(w_tail, rest_back)], axis=1)
    early = early + attended.astype(F32) + shared
    return final_sum(w_first.T, main_back, early)


def solution(mesh):
    finer = Mesh(mesh.devices.reshape(4, 4, 4, mesh.shape["tp"]), ("sp_0", "sp_1", "sp_2", "tp"))
    in_specs = (
        P(SP, "tp"),
        P(SP, "tp"),
        P(SP, "tp"),
        P(SP, "tp"),
        P(SP, "tp"),
        P(SP, "tp"),
        P("tp"),
        P(SP, "tp"),
        P(),
        P(),
        P(SP_TP, None),
        P(),
        P(SP_TP, None),
        P(SP_TP, None),
        P(SP_TP, None, None),
        P(SP_TP, None, None),
        P(SP_TP, None, None),
        P(),
        P(),
        P(),
    )
    out_specs = P(SP_TP, None)

    return jax.shard_map(
        shards, mesh=finer, in_specs=in_specs, out_specs=out_specs, check_vma=False
    )
```

```python
import functools

import jax
import jax.numpy as jnp
from jax import lax
from jax.experimental import pallas as pl
from jax.experimental.pallas import tpu as pltpu
from jax.sharding import Mesh
from jax.sharding import PartitionSpec as P

TOP_K = 4
HD = 128
BLOCK = 128
KEEP = 8
SP = ("sp_0", "sp_1", "sp_2")
SP_TP = ("sp_0", "sp_1", "sp_2", "tp")
EPS = 1e-06
F32 = jnp.float32
BF16 = jnp.bfloat16


def dot_nn(a, b):
    return lax.dot_general(a, b, (((1,), (0,)), ((), ())), preferred_element_type=F32)


def dot_nt(a, b):
    return lax.dot_general(a, b, (((1,), (1,)), ((), ())), preferred_element_type=F32)


def dot_tn(a, b):
    return lax.dot_general(a, b, (((0,), (0,)), ((), ())), preferred_element_type=F32)


def parts(x):
    high = x.astype(BF16)
    return high, (x - high.astype(F32)).astype(BF16)


def rows_of(*arrays):
    return jnp.concatenate(arrays, axis=0)


def cols_of(*arrays):
    return jnp.concatenate(arrays, axis=1)


def fine(a, b):
    ah, al = a
    bh, bl = b
    return dot_nn(cols_of(ah, al), rows_of(bh, bh)) + dot_nn(ah, bl)


def fine_square(a, b):
    ah, al = a
    bh, bl = b
    both = dot_nn(cols_of(ah, al), rows_of(cols_of(bh, bl), cols_of(bh, jnp.zeros_like(bl))))
    return both[:, :HD] + both[:, HD:]


def own_row(ref, head):
    table = ref[...].astype(F32)
    which = lax.broadcasted_iota(jnp.int32, table.shape, 0)
    return jnp.sum(jnp.where(which == head, table, 0.0), axis=0, keepdims=True)


def decay_sums(rate_ref, decay_ref, extra_ref, head):
    length = decay_ref.shape[1]
    raw = own_row(decay_ref, head) - 6.0
    soft = jnp.maximum(raw, 0.0) + jnp.log1p(jnp.exp(-jnp.abs(raw)))
    rate = jnp.exp(jnp.full((1, length), rate_ref[head], F32))
    total = jnp.broadcast_to(own_row(extra_ref, head) - rate * soft, (8, length))
    lane = lax.broadcasted_iota(jnp.int32, total.shape, 1)
    shift = 1
    while shift < length:
        total = total + jnp.where(lane >= shift, pltpu.roll(total, shift, 1), 0.0)
        shift *= 2
    g_row = total[0:1, :]
    return g_row, jnp.broadcast_to(g_row, (HD, length)).T


def unit(raw):
    x = raw.astype(F32)
    active = x * jax.nn.sigmoid(x)
    return active * lax.rsqrt(jnp.sum(active * active, axis=-1, keepdims=True) + EPS)


def against_keys(left, keys, number, g_row, g_col):
    ii = lax.broadcasted_iota(jnp.int32, (BLOCK, BLOCK), 0)
    jj = lax.broadcasted_iota(jnp.int32, (BLOCK, BLOCK), 1)
    blocks = []
    for r in range(number):
        here = slice(r * BLOCK, (r + 1) * BLOCK)
        upto = slice(0, (r + 1) * BLOCK)
        high = keys[0][upto]
        both = dot_nt(cols_of(left[0][here], left[1][here]), cols_of(high, high))
        both = both + dot_nt(left[0][here], keys[1][upto])
        row = []
        for c in range(r + 1):
            there = slice(c * BLOCK, (c + 1) * BLOCK)
            gap = g_col[here] - g_row[:, there]
            if c == r:
                gap = jnp.where(ii >= jj, gap, -1e30)
            row.append(both[:, there] * jnp.exp(gap))
        blocks.append(row)
    return blocks


PAIR = 2


def maps_kernel(place_ref, rate_ref, k_ref, v_ref, write_ref, decay_ref, extra_ref, *refs):
    map_refs, (high_ref, low_ref) = refs[:-2], refs[-2:]
    heads = len(map_refs)
    length = k_ref.shape[0]
    number = length // BLOCK
    ii = lax.broadcasted_iota(jnp.int32, (BLOCK, BLOCK), 0)
    jj = lax.broadcasted_iota(jnp.int32, (BLOCK, BLOCK), 1)
    eye = (ii == jj).astype(F32)
    pair = range(PAIR)
    heads_here = [pl.program_id(0) * PAIR + p for p in pair]
    lower, right, late, last = [], [], [], []
    for p in pair:
        there = slice(p * HD, (p + 1) * HD)
        g_row, g_col = decay_sums(rate_ref, decay_ref, extra_ref, heads_here[p])
        beta = jax.nn.sigmoid(own_row(write_ref, heads_here[p]))
        b_col = jnp.broadcast_to(beta, (HD, length)).T
        keys = unit(k_ref[:, there])
        raw = v_ref[:, there].astype(F32)
        values = raw * jax.nn.sigmoid(raw)
        k_beta = keys * b_col
        right.append(cols_of(k_beta * jnp.exp(g_col), values * b_col))
        last.append(g_col[length - 1 : length, :])
        late.append(parts(keys * jnp.exp(last[p] - g_col)))
        lower.append(against_keys(parts(k_beta), parts(keys), number, g_row, g_col))
    near = (ii // 2 == jj // 2) & (ii > jj)
    chains = [(p, r) for r in range(number) for p in pair]
    inverse = {(p, r): eye - jnp.where(near, lower[p][r][r], 0.0) for p, r in chains}
    for level in range(1, BLOCK.bit_length() - 1):
        chosen = (ii >> (level + 1) == jj >> (level + 1)) & (ii >> level > jj >> level)
        halves = {c: parts(inverse[c]) for c in chains}
        steps = {
            (p, r): fine_square(halves[p, r], parts(jnp.where(chosen, lower[p][r][r], 0.0)))
            for p, r in chains
        }
        inverse = {c: inverse[c] - fine_square(parts(steps[c]), halves[c]) for c in chains}
    highs, lows = [[] for _ in pair], [[] for _ in pair]
    for p, r in chains:
        here = slice(r * BLOCK, (r + 1) * BLOCK)
        there = slice(2 * p * HD, 2 * (p + 1) * HD)
        rest = right[p][here]
        if r > 0:
            known = (rows_of(*highs[p]), rows_of(*lows[p]))
            rest = rest - fine(parts(cols_of(*lower[p][r][:r])), known)
        one = parts(fine(parts(inverse[p, r]), parts(rest)))
        highs[p].append(one[0])
        lows[p].append(one[1])
        high_ref[here, there] = one[0]
        low_ref[here, there] = one[1]
    for p in pair:
        high, low = rows_of(*highs[p]), rows_of(*lows[p])
        moved = dot_tn(rows_of(*late[p]), rows_of(high, high)) + dot_tn(late[p][0], low)
        whole = cols_of(eye * jnp.exp(last[p]) - moved[:, :HD], moved[:, HD:])
        slot = (heads_here[p] + heads - place_ref[0]) % heads
        for s, map_ref in enumerate(map_refs):

            @pl.when(slot == s)
            def _(map_ref=map_ref, whole=whole):
                map_ref[...] = whole


def mixes_kernel(
    start, rate_ref, q_ref, k_ref, decay_ref, extra_ref, high_ref, low_ref, qe_ref, o0_ref
):
    length = q_ref.shape[0]
    number = length // BLOCK
    g_row, g_col = decay_sums(rate_ref, decay_ref, extra_ref, start + pl.program_id(0))
    queries = unit(q_ref[...])
    mixing = against_keys(parts(queries), parts(unit(k_ref[...])), number, g_row, g_col)
    grown = queries * jnp.exp(g_col)
    for r in range(number):
        here = slice(r * BLOCK, (r + 1) * BLOCK)
        upto = slice(0, (r + 1) * BLOCK)
        mixed = fine(parts(cols_of(*mixing[r])), (high_ref[upto, :], low_ref[upto, :]))
        qe_ref[here, :] = grown[here] - mixed[:, :HD]
        o0_ref[here, :] = mixed[:, HD:]


def state_maps(keys, values, write_logits, decays, rates, place):
    length, wide = keys.shape
    heads = wide // HD
    column = pl.BlockSpec((length, PAIR * HD), lambda step: (0, step))
    double = pl.BlockSpec((length, 2 * PAIR * HD), lambda step: (0, step))
    table = pl.BlockSpec((heads, length), lambda step: (0, 0))
    small = pl.BlockSpec(memory_space=pltpu.SMEM)
    one_map = pl.BlockSpec((HD, 2 * HD), lambda step: (0, 0))
    out = pl.pallas_call(
        maps_kernel,
        grid=(heads // PAIR,),
        in_specs=[small, small, column, column, table, table, table],
        out_specs=[one_map] * heads + [double, double],
        out_shape=[pltpu.VMEM((HD, 2 * HD), F32)] * heads
        + [jax.ShapeDtypeStruct((length, 2 * wide), BF16)] * 2,
        name="maps",
    )(place, rates, keys, values, write_logits.T, *decays)
    return out[:heads], out[heads], out[heads + 1]


def mixes(start, count, queries, keys, decays, rates, high, low):
    length, wide = queries.shape
    heads = wide // HD
    column = pl.BlockSpec((length, HD), lambda h: (0, start + h))
    double = pl.BlockSpec((length, 2 * HD), lambda h: (0, start + h))
    table = pl.BlockSpec((heads, length), lambda h: (0, 0))
    small = pl.BlockSpec(memory_space=pltpu.SMEM)
    return pl.pallas_call(
        functools.partial(mixes_kernel, start),
        grid=(count,),
        in_specs=[small, column, column, table, table, double, double],
        out_specs=[pl.BlockSpec((length, HD), lambda h: (0, h))] * 2,
        out_shape=[jax.ShapeDtypeStruct((length, count * HD), F32)] * 2,
        name="mixes",
    )(rates, queries, keys, *decays, high, low)


def shift_in(later):
    wide = lax.broadcasted_iota(jnp.int32, later.shape, 1)
    return jnp.where(wide >= HD, later, 0.0)


def then(later, earlier):
    return fine(parts(later[:, :HD]), parts(earlier)) + shift_in(later)


def identity_map():
    ii = lax.broadcasted_iota(jnp.int32, (HD, 2 * HD), 0)
    jj = lax.broadcasted_iota(jnp.int32, (HD, 2 * HD), 1)
    return (ii == jj).astype(F32)


def in_order(place, refs, held_ref):
    number = len(refs)
    for s, ref in enumerate(refs):
        held_ref[(place + number - s) % number] = ref[...]


def all_before_kernel(place_ref, *refs):
    maps, (before_ref, total_ref, held_ref) = refs[:-3], refs[-3:]
    in_order(place_ref[0], maps, held_ref)
    running = identity_map()
    for k in range(len(maps)):
        before_ref[k] = running
        running = held_ref[k] if k == 0 else then(held_ref[k], running)
    total_ref[...] = running


def mine_before_kernel(place_ref, *refs):
    maps, (before_ref, total_ref, held_ref) = refs[:-3], refs[-3:]
    place = place_ref[0]
    in_order(place, maps, held_ref)
    running = identity_map()
    before_ref[...] = running
    for k in range(len(maps)):
        running = held_ref[k] if k == 0 else then(held_ref[k], running)

        @pl.when(place == k + 1)
        def _(running=running):
            before_ref[...] = running

    total_ref[...] = running


def small_call(kernel, out_shape, scratch, place, *arrays):
    return pl.pallas_call(
        kernel,
        in_specs=[pl.BlockSpec(memory_space=pltpu.SMEM)]
        + [pl.BlockSpec(memory_space=pltpu.VMEM)] * len(arrays),
        out_shape=out_shape,
        scratch_shapes=scratch,
        compiler_params=pltpu.CompilerParams(vmem_limit_bytes=8 << 20),
    )(place, *[pltpu.with_memory_space_constraint(a, pltpu.VMEM) for a in arrays])


def states_kernel(place_ref, one_ref, two_ref, three_ref, middle_ref, inner_ref, *out_refs):
    state = three_ref[:, HD:]
    for ref in (two_ref, one_ref, middle_ref):
        state = fine(parts(ref[:, :HD]), parts(state)) + ref[:, HD:]
    pair = parts(state)
    number = len(out_refs)
    for s, out_ref in enumerate(out_refs):
        k = (place_ref[0] + number - s) % number
        out_ref[...] = fine(parts(inner_ref[k, :, :HD]), pair) + inner_ref[k, :, HD:]


def ring(array, axis, step):
    count = lax.axis_size(axis)
    return lax.ppermute(array, axis, [(i, (i + step) % count) for i in range(count)])


def onward(array, axis, step):
    count = lax.axis_size(axis)
    return lax.ppermute(array, axis, [(i, i + step) for i in range(count - step)])


def place_on(axis):
    return lax.axis_index(axis).reshape(1).astype(jnp.int32)


def entering(own, arrived, place):
    number = 1 + len(arrived)
    one = pltpu.VMEM(own.shape, F32)
    many = pltpu.VMEM((number,) + own.shape, F32)
    held = [pltpu.VMEM((number,) + own.shape, F32)]
    inner, line = small_call(all_before_kernel, [many, one], held, place, own, *arrived)
    two = ring(line, "sp_1", 2)
    first, three = [ring(line, "sp_1", s) for s in (1, 3)]
    middle, plane = small_call(
        mine_before_kernel, [one, one], held, place_on("sp_1"), line, first, two, three
    )
    two = onward(plane, "sp_0", 2)
    first, three = [onward(plane, "sp_0", s) for s in (1, 3)]
    found = small_call(
        states_kernel,
        [pltpu.VMEM((HD, HD), F32)] * number,
        (),
        place,
        first,
        two,
        three,
        middle,
        inner,
    )
    two, first, three = [ring(found[s], "sp_2", number - s) for s in (2, 1, 3)]
    return [found[0], first, two, three]


def finish_kernel(place_ref, core_ref, gain_ref, *refs):
    states, refs = refs[:-12], refs[-12:]
    mixed_hbm, (gate_hbm, keep_ref, send_ref) = refs[:4], refs[4:7]
    qe_ref, o0_ref, gate_ref, whole_ref, done = refs[7:]
    number = len(states)
    half = keep_ref.shape[0]
    core = core_ref[0]
    targets = (qe_ref, o0_ref, gate_ref)
    each = number // 2

    def arrival(i, h, source, column):
        there = pl.ds(pl.multiple_of(h * HD, HD), HD)
        here = pl.ds(pl.multiple_of(column * HD, HD), HD)
        return pltpu.make_async_copy(source.at[:, here], targets[i].at[:, there], done.at[i, h])

    for h in range(number):
        for i in range(2):
            arrival(i, h, mixed_hbm[2 * (h // each) + i], h % each).start()
        arrival(2, h, gate_hbm, h).start()

    @pl.loop(0, number)
    def _(h):
        there = pl.ds(pl.multiple_of(h * HD, HD), HD)
        slot = (h + number - place_ref[0]) % number
        state = states[0][...]
        for s in range(1, number):
            state = jnp.where(slot == s, states[s][...], state)
        for i in range(2):
            arrival(i, h, mixed_hbm[i], 0).wait()
        arrival(2, h, gate_hbm, h).wait()
        mix = o0_ref[:, there] + fine(parts(qe_ref[:, there]), parts(state))
        scaled = mix * lax.rsqrt(jnp.mean(mix * mix, axis=-1, keepdims=True) + EPS)
        gate = gate_ref[:, there].astype(F32)
        whole_ref[...] = scaled * gain_ref[...] * (gate * jax.nn.sigmoid(gate))
        keep_ref[:, there] = whole_ref[pl.ds(core * half, half), :].astype(BF16)
        send_ref[:, there] = whole_ref[pl.ds((1 - core) * half, half), :].astype(BF16)


def finish(mixed, states, gate, gain, place):
    length, wide = gate.shape
    small = pl.BlockSpec(memory_space=pltpu.SMEM)
    arrays = (gain.reshape(1, HD), *states)
    return pl.pallas_call(
        finish_kernel,
        in_specs=[small, small]
        + [pl.BlockSpec(memory_space=pltpu.VMEM)] * len(arrays)
        + [pl.BlockSpec(memory_space=pl.ANY)] * 5,
        out_shape=[pltpu.VMEM((length // 2, wide), BF16)] * 2,
        scratch_shapes=[
            pltpu.VMEM((length, wide), F32),
            pltpu.VMEM((length, wide), F32),
            pltpu.VMEM((length, wide), BF16),
            pltpu.VMEM((length, HD), F32),
            pltpu.SemaphoreType.DMA((3, len(states))),
        ],
        compiler_params=pltpu.CompilerParams(vmem_limit_bytes=12 << 20),
        name="finish",
    )(
        place,
        place_on("tp"),
        *[pltpu.with_memory_space_constraint(a, pltpu.VMEM) for a in arrays],
        *[pltpu.with_memory_space_constraint(a, pltpu.HBM) for a in (*mixed, gate)],
    )


def feed_forward(rows, w_gate, w_up, w_down):
    hidden = jax.nn.silu(jnp.dot(rows, w_gate, preferred_element_type=F32))
    hidden = (hidden * jnp.dot(rows, w_up, preferred_element_type=F32)).astype(BF16)
    return jnp.dot(hidden, w_down, preferred_element_type=F32)


def exchange(rows):
    return lax.all_to_all(rows, SP_TP, split_axis=0, concat_axis=0, tiled=True)


def slots_of(index, experts):
    length = index.shape[0]
    ids = jnp.arange(experts, dtype=jnp.int32)[:, None]
    named = jnp.zeros((experts, length), F32)
    for j in range(index.shape[1]):
        named = named + (index[:, j][None, :] == ids).astype(F32)
    place = jnp.arange(length, dtype=jnp.int32)
    earlier = (place[:, None] < place[None, :]).astype(BF16)
    before = jnp.dot(named.astype(BF16), earlier, preferred_element_type=F32)
    return jnp.where(named > 0, before, -1.0)


def tables_of(index, weight, slot, room):
    experts, length = slot.shape
    ids = jnp.arange(experts, dtype=jnp.int32)[:, None]
    weights = jnp.zeros((experts, length), F32)
    for j in range(index.shape[1]):
        weights = weights + jnp.where(
            index[:, j][None, :] == ids, weight[:, j][None, :], 0.0
        )
    weights, slot = weights[:, None, :], slot[:, None, :]
    step = jnp.arange(KEEP, dtype=jnp.int32)[None, :, None]
    extra = room - KEEP
    rest = slot == (KEEP + step % extra).astype(F32)
    masks = (slot == step.astype(F32), rest & (step < extra), rest & (step >= extra))
    return [
        jnp.where(m, weights, 0.0).astype(BF16).reshape(experts * KEEP, length) for m in masks
    ]


def places(slot_ref, start, count, length):
    slot = slot_ref[pl.ds(start, count), :]
    slot = jnp.broadcast_to(slot[:, None, :], (count, KEEP, length)).reshape(count * KEEP, length)
    step = lax.broadcasted_iota(jnp.int32, (count * KEEP, length), 0) % KEEP
    return slot, step


def matrix_chunks(half, matrix_ref, matrix_vmem, done):
    number = done.shape[0]
    wide, dim = matrix_vmem.shape
    rows = pl.ds(pl.multiple_of(half * wide, wide), wide)
    spans = [slice(c * dim // number, (c + 1) * dim // number) for c in range(number)]
    copies = [
        pltpu.make_async_copy(matrix_ref.at[rows, s], matrix_vmem.at[:, s], done.at[c])
        for c, s in enumerate(spans)
    ]
    return list(zip(spans, copies, strict=True))


def own_half_kernel(core_ref, keep_ref, matrix_ref, out_ref, matrix_vmem, done):
    chunks = matrix_chunks(core_ref[0], matrix_ref, matrix_vmem, done)
    for _, copy in chunks:
        copy.start()
    for there, copy in chunks:
        copy.wait()
        out_ref[:, there] = dot_nn(keep_ref[...], matrix_vmem[:, there])


def own_half(keep, out_matrix):
    length, wide = keep.shape
    dim = out_matrix.shape[1]
    return pl.pallas_call(
        own_half_kernel,
        in_specs=[
            pl.BlockSpec(memory_space=pltpu.SMEM),
            pl.BlockSpec(memory_space=pltpu.VMEM),
            pl.BlockSpec(memory_space=pl.ANY),
        ],
        out_shape=pltpu.VMEM((length, dim), F32),
        scratch_shapes=[pltpu.VMEM((wide, dim), BF16), pltpu.SemaphoreType.DMA((4,))],
        compiler_params=pltpu.CompilerParams(vmem_limit_bytes=8 << 20),
        name="own_half",
    )(
        place_on("tp"),
        pltpu.with_memory_space_constraint(keep, pltpu.VMEM),
        pltpu.with_memory_space_constraint(out_matrix, pltpu.HBM),
    )


def attend_kernel(
    core_ref, own_ref, came_ref, gain_ref, slot_ref, matrix_ref, residual_ref, *refs
):
    attended_hbm, normed_hbm, rest_hbm, attended_ref, normed_ref, rest_ref = refs[:6]
    wide_ref, matrix_vmem, residual_vmem, lead_ref, tail_ref, ready, done, gone = refs[6:]
    length, dim = residual_ref.shape
    count = 32
    residual_comes = pltpu.make_async_copy(residual_ref, residual_vmem, ready.at[0])
    chunks = matrix_chunks(1 - core_ref[0], matrix_ref, matrix_vmem, done)
    residual_comes.start()
    for _, copy in chunks:
        copy.start()

    @pl.loop(0, slot_ref.shape[0] // count)
    def _(i):
        start = pl.multiple_of(i * count, count)
        there = pl.ds(pl.multiple_of(i * count * KEEP, count * KEEP), count * KEEP)
        slot, step = places(slot_ref, start, count, length)
        extra = KEEP // 2
        chosen = slot == (KEEP + step % extra).astype(F32)
        lead_ref[there, :] = (chosen & (step < extra)).astype(F32).astype(BF16)
        tail_ref[there, :] = (chosen & (step >= extra)).astype(F32).astype(BF16)

    residual_comes.wait()
    squares = jnp.zeros((length, 1), F32)
    for there, copy in chunks:
        copy.wait()
        projected = own_ref[:, there] + dot_nn(came_ref[...], matrix_vmem[:, there])
        attended = (residual_vmem[:, there].astype(F32) + projected).astype(BF16)
        attended_ref[:, there] = attended
        plain = attended.astype(F32)
        wide_ref[:, there] = plain
        squares = squares + jnp.sum(plain * plain, axis=-1, keepdims=True)
    leaving = [pltpu.make_async_copy(attended_ref, attended_hbm, gone.at[0])]
    leaving[0].start()
    scale = lax.rsqrt(squares / dim + EPS)
    normed_ref[...] = (wide_ref[...] * scale * gain_ref[...]).astype(BF16)
    leaving.append(pltpu.make_async_copy(normed_ref, normed_hbm, gone.at[1]))
    leaving[1].start()
    half = dim // 2

    def departure(i):
        there = pl.ds(pl.multiple_of(i * count, count), count)
        return pltpu.make_async_copy(rest_ref.at[there], rest_hbm.at[there], gone.at[2 + i])

    @pl.loop(0, slot_ref.shape[0] // count)
    def _(i):
        start = pl.multiple_of(i * count, count)
        there = pl.ds(pl.multiple_of(i * count * KEEP, count * KEEP), count * KEEP)
        lead, tail = lead_ref[there, :], tail_ref[there, :]
        rows = dot_nn(lead, normed_ref[:, :half]) + dot_nn(tail, normed_ref[:, half:])
        rest_ref[pl.ds(start, count), :, :] = rows.astype(BF16).reshape(count, KEEP, half)
        departure(i).start()

    for i in range(slot_ref.shape[0] // count):
        departure(i).wait()
    for copy in leaving:
        copy.wait()


def attend(own, came, out_matrix, residual, gain, slot):
    length, dim = residual.shape
    experts = slot.shape[0]
    arrays = (own, came, gain.reshape(1, dim), slot)
    rows = pltpu.HBM((length, dim), BF16)
    return pl.pallas_call(
        attend_kernel,
        in_specs=[pl.BlockSpec(memory_space=pltpu.SMEM)]
        + [pl.BlockSpec(memory_space=pltpu.VMEM)] * len(arrays)
        + [pl.BlockSpec(memory_space=pl.ANY)] * 2,
        out_specs=[pl.BlockSpec(memory_space=pl.ANY)] * 3,
        out_shape=[rows, rows, pltpu.HBM((experts, KEEP, dim // 2), BF16)],
        scratch_shapes=[
            pltpu.VMEM((length, dim), BF16),
            pltpu.VMEM((length, dim), BF16),
            pltpu.VMEM((experts, KEEP, dim // 2), BF16),
            pltpu.VMEM((length, dim), F32),
            pltpu.VMEM((came.shape[1], dim), BF16),
            pltpu.VMEM((length, dim), BF16),
            pltpu.VMEM((experts * KEEP, length), BF16),
            pltpu.VMEM((experts * KEEP, length), BF16),
            pltpu.SemaphoreType.DMA((1,)),
            pltpu.SemaphoreType.DMA((4,)),
            pltpu.SemaphoreType.DMA((2 + experts // 32,)),
        ],
        compiler_params=pltpu.CompilerParams(vmem_limit_bytes=20 << 20),
        name="attend",
    )(
        place_on("tp"),
        *[pltpu.with_memory_space_constraint(a, pltpu.VMEM) for a in arrays],
        *[pltpu.with_memory_space_constraint(a, pltpu.HBM) for a in (out_matrix, residual)],
    )


def dispatch_kernel(slot_ref, normed_ref, out_ref):
    count, _, dim = out_ref.shape
    start = pl.multiple_of(pl.program_id(0) * count, count)
    slot, step = places(slot_ref, start, count, normed_ref.shape[0])
    chosen = (slot == step.astype(F32)).astype(F32).astype(BF16)
    rows = dot_nn(chosen, normed_ref[...]).astype(BF16)
    out_ref[...] = rows.reshape(count, KEEP, dim)


def dispatch(slot, normed):
    experts, length = slot.shape
    dim = normed.shape[1]
    count = 16
    return pl.pallas_call(
        dispatch_kernel,
        grid=(experts // count,),
        in_specs=[
            pl.BlockSpec((experts, length), lambda i: (0, 0)),
            pl.BlockSpec((length, dim), lambda i: (0, 0)),
        ],
        out_specs=pl.BlockSpec((count, KEEP, dim), lambda i: (i, 0, 0)),
        out_shape=jax.ShapeDtypeStruct((experts, KEEP, dim), BF16),
        name="dispatch",
    )(slot, normed)


def final_kernel(table_ref, early_ref, rows_ref, out_ref, early_vmem, rows_vmem, out_vmem, done):
    number = done.shape[1]
    block = out_vmem.shape[1] // number
    spans = [pl.ds(c * block, block) for c in range(number)]
    comes = [
        pltpu.make_async_copy(rows_ref.at[:, s], rows_vmem.at[:, s], done.at[0, c])
        for c, s in enumerate(spans)
    ]
    goes = [
        pltpu.make_async_copy(out_vmem.at[:, s], out_ref.at[:, s], done.at[1, c])
        for c, s in enumerate(spans)
    ]
    sums = [
        pltpu.make_async_copy(early_ref.at[:, s], early_vmem.at[:, s], done.at[2, c])
        for c, s in enumerate(spans)
    ]
    for c in range(number):
        comes[c].start()
        sums[c].start()
    for c in range(number):
        there = slice(c * block, (c + 1) * block)
        comes[c].wait()
        sums[c].wait()
        total = early_vmem[:, there] + dot_nn(table_ref[...], rows_vmem[:, there])
        out_vmem[:, there] = total.astype(BF16)
        goes[c].start()
    for copy in goes:
        copy.wait()


def final_sum(table, rows, early):
    length, wide = early.shape
    return pl.pallas_call(
        final_kernel,
        in_specs=[pl.BlockSpec(memory_space=pltpu.VMEM)] + [pl.BlockSpec(memory_space=pl.ANY)] * 2,
        out_specs=pl.BlockSpec(memory_space=pl.ANY),
        out_shape=pltpu.HBM((length, wide), BF16),
        scratch_shapes=[
            pltpu.VMEM((length, wide), F32),
            pltpu.VMEM(rows.shape, BF16),
            pltpu.VMEM((length, wide), BF16),
            pltpu.SemaphoreType.DMA((3, 8)),
        ],
        compiler_params=pltpu.CompilerParams(vmem_limit_bytes=16 << 20),
        name="final_sum",
    )(
        pltpu.with_memory_space_constraint(table, pltpu.VMEM),
        *[pltpu.with_memory_space_constraint(a, pltpu.HBM) for a in (early, rows)],
    )


def shards(
    projected_queries,
    projected_keys,
    projected_values,
    output_gate_values,
    write_strength_logits,
    decay_input_logits,
    head_rate_logarithm,
    extra_log_decay,
    per_head_norm_gain,
    output_matrix,
    residual,
    mixture_norm_gain,
    selected_expert_index,
    routing_weight,
    routed_gate_weight,
    routed_up_weight,
    routed_down_weight,
    common_gate_weight,
    common_up_weight,
    common_down_weight,
):
    place = place_on("sp_2")
    decays = (decay_input_logits.T, extra_log_decay.T)
    (own, near, far, last), high, low = state_maps(
        projected_keys,
        projected_values,
        write_strength_logits,
        decays,
        head_rate_logarithm,
        place,
    )
    far = ring(far, "sp_2", 2)
    near, last = ring(near, "sp_2", 1), ring(last, "sp_2", 3)
    states = entering(own, (near, far, last), place)
    pieces = (projected_queries, projected_keys, decays, head_rate_logarithm, high, low)
    count = len(states) // 2
    mixed = tuple(mixes(0, count, *pieces))
    mixed = mixed + tuple(mixes(count, count, *pieces))
    keep, send = finish(mixed, states, output_gate_values, per_head_norm_gain, place)
    came = ring(send, "tp", 1)
    own = own_half(keep, output_matrix)
    length, dim = residual.shape
    experts = lax.axis_size(SP) * lax.axis_size("tp")
    room = max(2, length * TOP_K * 3 // (2 * experts))
    extra = room - KEEP
    half = dim // 2
    slot = slots_of(selected_expert_index, experts)
    w_first, w_lead, w_tail = tables_of(selected_expert_index, routing_weight, slot, room)
    attended, normed, rest_out = attend(own, came, output_matrix, residual, mixture_norm_gain, slot)
    rest_in = exchange(rest_out)
    main_in = exchange(dispatch(slot, normed))
    shared = feed_forward(normed, common_gate_weight, common_up_weight, common_down_weight)

    weights = (routed_gate_weight[0], routed_up_weight[0], routed_down_weight[0])
    main_rows = feed_forward(main_in.reshape(experts * KEEP, dim), *weights).astype(BF16)
    main_back = exchange(main_rows.reshape(experts, KEEP, dim)).reshape(experts * KEEP, dim)
    unfolded = rest_in.reshape(experts, 2, extra, half).transpose(0, 2, 1, 3)
    rest_rows = feed_forward(unfolded.reshape(experts * extra, dim), *weights).astype(BF16)
    folded = rest_rows.reshape(experts, extra, 2, half).transpose(0, 2, 1, 3)
    rest_back = exchange(folded.reshape(experts, KEEP, half)).reshape(experts * KEEP, half)

    def combine(table, rows):
        return lax.dot_general(table, rows, (((0,), (0,)), ((), ())), preferred_element_type=F32)

    early = jnp.concatenate([combine(w_lead, rest_back), combine(w_tail, rest_back)], axis=1)
    early = early + attended.astype(F32) + shared
    return final_sum(w_first.T, main_back, early)


def solution(mesh):
    finer = Mesh(mesh.devices.reshape(4, 4, 4, mesh.shape["tp"]), ("sp_0", "sp_1", "sp_2", "tp"))
    in_specs = (
        P(SP, "tp"),
        P(SP, "tp"),
        P(SP, "tp"),
        P(SP, "tp"),
        P(SP, "tp"),
        P(SP, "tp"),
        P("tp"),
        P(SP, "tp"),
        P(),
        P(),
        P(SP_TP, None),
        P(),
        P(SP_TP, None),
        P(SP_TP, None),
        P(SP_TP, None, None),
        P(SP_TP, None, None),
        P(SP_TP, None, None),
        P(),
        P(),
        P(),
    )
    out_specs = P(SP_TP, None)

    return jax.shard_map(
        shards, mesh=finer, in_specs=in_specs, out_specs=out_specs, check_vma=False
    )
```
